256 devices in a mesh: sp: 32 (over z, x), tp: 8 (over y, core).
Axes of the slice: x: 4, y: 4, z: 8, core: 2. Of those that a mesh axis runs over, the one named last changes fastest.
Arguments:
- out_grad: bfloat16 [4096, 2048], P('sp', 'tp'), may hold values from -6 to 6
- moe_input: bfloat16 [4096, 2048], P('sp', 'tp'), may hold values from -6 to 6
- route_weight: float32 [4096, 2], P('sp'), may hold values from 0.2 to 1
- route_ids: int32 [4096, 2], P('sp'), may hold values from 0 to 31, all different within a row; in each aligned block of 128 rows (0 to 127, 128 to 255, ...) at most 16 rows name the same one
- gate_proj: bfloat16 [32, 2048, 2816], P('sp', None, 'tp'), may hold values from -0.125 to 0.125
- up_proj: bfloat16 [32, 2048, 2816], P('sp', None, 'tp'), may hold values from -0.125 to 0.125
- down_proj: bfloat16 [32, 2816, 2048], P('sp', 'tp'), may hold values from -0.109375 to 0.109375
- out_proj: bfloat16 [2048, 2048], P(None, 'tp'), may hold values from -0.125 to 0.125
- conv_out: bfloat16 [4096, 2048], P('sp', 'tp'), may hold values from -6 to 6
- gate_b: bfloat16 [4096, 2048], P('sp', 'tp'), may hold values from -6 to 6
- gate_c: bfloat16 [4096, 2048], P('sp', 'tp'), may hold values from -6 to 6
- value_v: bfloat16 [4096, 2048], P('sp', 'tp'), may hold values from -6 to 6
- conv_taps: float32 [3, 2048], P(None, 'tp'), may hold values from -3 to 3
Outputs:
- grad_gate: bfloat16 [32, 2048, 2816], P('sp', None, 'tp')
- grad_up: bfloat16 [32, 2048, 2816], P('sp', None, 'tp')
- grad_down: bfloat16 [32, 2816, 2048], P('sp', 'tp')
- grad_out: float32 [2048, 2048], P('sp', 'tp')
- grad_b: bfloat16 [4096, 2048], P('sp', 'tp')
- grad_c: bfloat16 [4096, 2048], P('sp', 'tp')
- grad_v: bfloat16 [4096, 2048], P('sp', 'tp')
The draws below stay inside these ranges and needn't reach their ends.
Inputs may be any that keep to these rules, and one draw needn't show every extreme that they name: `route_ids`: each row names two different experts; within the 128 rows of one index of sp no expert is named by more than 16 rows, a bound that some block reaches.
All inputs are finite; a program needn't handle non-finite values.
Results may differ from the reference program's by a relative error of at most 0.019.
Values may be sent and summed in bfloat16 or wider, within the bound.
A program may use at most 64 MiB of HBM per device.

```python
import math
import jax
import jax.numpy as jnp
import numpy as np
from jax import lax

D = 2048
FF = 2816
TOK_DEV = 128
TOKENS = 4096
EXPERTS = 32
CAP = 16
N_SP = 32
N_TP = 8


def with_spikes(drawn, key, source, target, shards_of, factor):
    owner, partner = [(jnp.arange(drawn.shape[axis_at]) // (drawn.shape[axis_at] // shards_of)).reshape([-1 if axis == axis_at else 1 for axis in range(drawn.ndim)]) for axis_at in (source, target)]
    chosen = jax.random.permutation(key, shards_of)[partner]
    strong = (owner == chosen) | (owner == (partner + shards_of // 2) % shards_of)
    return jnp.where(strong, factor * drawn, drawn)


def block_levels(rng, shape, pieces, smallest, top_value):
    def one(axis_at, blocks):
        heights = jax.random.uniform(jax.random.fold_in(jax.random.fold_in(rng, 6), axis_at), (blocks,), jnp.float32, smallest / len(pieces), top_value / len(pieces))
        return jnp.repeat(jnp.exp(heights), shape[axis_at] // blocks).reshape((-1,) + (1,) * (len(shape) - axis_at - 1))

    level = one(*pieces[0])
    for cut in pieces[1:]:
        level = level * one(*cut)
    return level


def routed_block(key, own, number, rows, amount, top, bound, skew):
    order = jax.random.permutation(key, amount)
    crowded, ordinary = portions_of(amount, rows * top, bound, skew, True), portions_of(amount, rows * top, bound, skew, False)
    places = jnp.arange(amount)

    def named(sizes, rotation):
        used = int((sizes > 0).sum())
        fixed = max(1, used // 4)
        passed = fixed + (places - fixed + rotation * (used - fixed)) % max(1, amount - fixed)
        return jnp.zeros((amount,), jnp.int32).at[order[jnp.where(places < fixed, places, passed)]].set(jnp.asarray(sizes, jnp.int32))

    sizes = jnp.where(number % 4 == 0, named(crowded, number // 4), named(ordinary, number - number // 4 - 1))
    mixed = jax.random.permutation(jax.random.fold_in(own, 3), amount)
    donor, sink = mixed[0:amount // 2 * 2:2], mixed[1:amount // 2 * 2:2]
    room = jnp.minimum(sizes[donor] - 1, bound - sizes[sink]) // 2
    room = jnp.where((donor == order[0]) | (sink == order[0]) | (sizes[sink] == 0), 0, jnp.maximum(room, 0))
    passed = jax.random.randint(jax.random.fold_in(own, 4), (amount // 2,), 0, 1 << 20) % (room + 1)
    sizes = sizes.at[donor].add(-passed).at[sink].add(passed)
    labels = jnp.searchsorted(jnp.cumsum(sizes), jnp.arange(rows * top), side="right").astype(jnp.int32)
    grid = labels.reshape(top, rows).T
    grid = grid[jax.random.permutation(jax.random.fold_in(own, 1), rows)]
    rotation = jax.random.randint(jax.random.fold_in(own, 2), (rows, 1), 0, top)
    return jnp.take_along_axis(grid, (jnp.arange(top)[None, :] + rotation) % top, axis=1)


def portions_of(count, total, most, skew, full):
    weights = [(1 << 20) // math.isqrt(standing ** skew) + 1 for standing in range(1, count + 1)]
    largest = most if full else min(most, max(-(-total // count), total * weights[0] // sum(weights)))
    least = 1 if total - largest >= count - 1 else 0
    given, surplus = [largest] + [least] * (count - 1), total - largest - least * (count - 1)
    while surplus > 0:
        movable = [i for i in range(1, count) if given[i] < largest] or [i for i in range(1, count) if given[i] < most]
        mass, left = sum([weights[i] for i in movable]), surplus
        for i in movable:
            addition = min(most - given[i], max(1, left * weights[i] // mass), surplus)
            given[i] = given[i] + addition
            surplus = surplus - addition
    return np.array(given)


def normal_values(rng, shape, deviation, reach, split=(), kind=jnp.bfloat16):
    loudness = block_levels(rng, shape, split, -0.22, 0.18) if split else 1.0
    values = jax.random.normal(rng, shape, jnp.float32) * deviation * loudness
    return jnp.minimum(jnp.maximum(values, -reach), reach).astype(kind)


def bell_draw_with(rng, extent, spread, limit, pieces, heavy, held_as=jnp.bfloat16):
    array = spread * jax.random.normal(rng, extent, jnp.float32)
    if pieces:
        array = array * block_levels(rng, extent, pieces, -0.22, 0.18)
    return jnp.clip(with_spikes(array, jax.random.fold_in(rng, 3), *heavy), -limit, limit).astype(held_as)


def setup_inputs(seed: int = 0) -> dict:
    arg_keys = jax.random.split(jax.random.key(seed), 14)
    out_grad = bell_draw_with(arg_keys[0], (TOKENS, D), 1.0, 6.0, ((0, 32), (1, 8)), (0, 1, 32, 2.75))
    moe_input = normal_values(arg_keys[1], (TOKENS, D), 1.0, 6.0, ((0, 32), (1, 8)))
    route_weight = jnp.clip(jnp.exp(math.log(1.0) - 1.609438 * jax.random.uniform(arg_keys[2], (TOKENS, 2), jnp.float32) ** block_levels(arg_keys[2], (TOKENS, 2), ((0, 32),), -0.2, 0.2)), 0.2, 1.0)
    route_ids_keys = jax.random.split(jax.random.fold_in(arg_keys[3], 1), TOKENS // TOK_DEV)
    route_ids_turns = jax.random.permutation(jax.random.fold_in(arg_keys[3], 3), TOKENS // TOK_DEV)
    route_ids = jax.vmap(lambda own, number: routed_block(jax.random.fold_in(arg_keys[3], 2), own, number, TOK_DEV, EXPERTS, 2, CAP, 1))(route_ids_keys, route_ids_turns).reshape((TOKENS, 2))
    gate_proj = normal_values(arg_keys[4], (EXPERTS, D, FF), D ** -0.5, 0.125, ((0, 32), (2, 8)))
    up_proj = normal_values(arg_keys[5], (EXPERTS, D, FF), D ** -0.5, 0.125, ((0, 32), (2, 8)))
    down_proj = normal_values(arg_keys[6], (EXPERTS, FF, D), FF ** -0.5, 0.109375, ((0, 32), (1, 8)))
    out_proj = normal_values(arg_keys[7], (D, D), D ** -0.5, 0.125, ((1, 8),))
    conv_out = normal_values(arg_keys[8], (TOKENS, D), 1.0, 6.0, ((0, 32), (1, 8)))
    gate_b = normal_values(arg_keys[9], (TOKENS, D), 1.0, 6.0, ((0, 32), (1, 8)))
    gate_c = normal_values(arg_keys[10], (TOKENS, D), 1.0, 6.0, ((0, 32), (1, 8)))
    value_v = normal_values(arg_keys[11], (TOKENS, D), 1.0, 6.0, ((0, 32), (1, 8)))
    conv_taps = normal_values(arg_keys[12], (3, D), 0.6, 3.0, ((1, 8),), jnp.float32)
    return {"out_grad": out_grad, "moe_input": moe_input, "route_weight": route_weight, "route_ids": route_ids, "gate_proj": gate_proj, "up_proj": up_proj, "down_proj": down_proj, "out_proj": out_proj, "conv_out": conv_out, "gate_b": gate_b, "gate_c": gate_c, "value_v": value_v, "conv_taps": conv_taps}


def slot_table(route_ids):
    flat = route_ids.reshape(N_SP, TOK_DEV * 2).astype(jnp.int32)
    onehot = (flat[:, :, None] == jnp.arange(EXPERTS, dtype=jnp.int32)[None, None, :]).astype(jnp.int32)
    before = jnp.cumsum(onehot, axis=1) - onehot
    slot = jnp.sum(before * onehot, axis=2).astype(jnp.int32)
    return (flat * CAP + slot).astype(jnp.int32)


def place_rows(rows, index):
    return jnp.zeros((EXPERTS * CAP, rows.shape[1]), rows.dtype).at[index].set(rows)


def reference(out_grad, moe_input, route_weight, route_ids, gate_proj, up_proj, down_proj, out_proj, conv_out, gate_b, gate_c, value_v, conv_taps):
    dest = slot_table(route_ids)
    sent = (route_weight[:, :, None] * out_grad.astype(jnp.float32)[:, None, :]).astype(jnp.bfloat16)
    rows_x = jnp.broadcast_to(moe_input[:, None, :], (TOKENS, 2, D)).reshape(N_SP, 2 * TOK_DEV, D)
    rows_dy = sent.reshape(N_SP, 2 * TOK_DEV, D)
    slots_x = jax.vmap(place_rows)(rows_x, dest).reshape(N_SP, EXPERTS, CAP, D)
    slots_dy = jax.vmap(place_rows)(rows_dy, dest).reshape(N_SP, EXPERTS, CAP, D)
    width = FF // N_TP

    def expert(index):
        xin = slots_x[:, index].reshape(N_SP * CAP, D)
        dyin = slots_dy[:, index].reshape(N_SP * CAP, D)
        w_gate = gate_proj[index]
        w_up = up_proj[index]
        w_down = down_proj[index]
        gate = jnp.dot(xin, w_gate, preferred_element_type=jnp.float32)
        upval = jnp.dot(xin, w_up, preferred_element_type=jnp.float32)
        sig = jax.nn.sigmoid(gate)
        act = gate * sig
        hidden = (act * upval).astype(jnp.bfloat16)
        g_down = jnp.dot(hidden.T, dyin, preferred_element_type=jnp.float32).astype(jnp.bfloat16)
        dhid = jnp.dot(dyin, w_down.T, preferred_element_type=jnp.float32)
        dgate = (dhid * upval * (sig * (1.0 + gate * (1.0 - sig)))).astype(jnp.bfloat16)
        dup = (dhid * act).astype(jnp.bfloat16)
        g_gate = jnp.dot(xin.T, dgate, preferred_element_type=jnp.float32).astype(jnp.bfloat16)
        g_up = jnp.dot(xin.T, dup, preferred_element_type=jnp.float32).astype(jnp.bfloat16)
        rows = N_SP * CAP
        part = jnp.einsum('rpf,dpf->prd', dgate.reshape(rows, N_TP, width).astype(jnp.float32),
                          w_gate.reshape(D, N_TP, width).astype(jnp.float32))
        part = part + jnp.einsum('rpf,dpf->prd', dup.reshape(rows, N_TP, width).astype(jnp.float32),
                                 w_up.reshape(D, N_TP, width).astype(jnp.float32))
        part = lax.optimization_barrier(part.astype(jnp.bfloat16)).astype(jnp.float32)
        back = jnp.sum(part, axis=0).astype(jnp.bfloat16)
        return g_gate, g_up, g_down, back

    grad_gate, grad_up, grad_down, backs = lax.map(expert, jnp.arange(EXPERTS, dtype=jnp.int32))
    backs = backs.reshape(EXPERTS, N_SP, CAP, D).transpose(1, 0, 2, 3).reshape(N_SP, EXPERTS * CAP, D)
    picked = jax.vmap(lambda table, index: table[index])(backs, dest)
    moe_grad = jnp.sum(picked.reshape(TOKENS, 2, D).astype(jnp.float32), axis=1)
    grad_h = (out_grad.astype(jnp.float32) + moe_grad).astype(jnp.bfloat16)
    grad_z = jnp.dot(grad_h, out_proj, preferred_element_type=jnp.float32)
    dconv = (grad_z * gate_b.astype(jnp.float32)).astype(jnp.bfloat16)
    grad_b = (grad_z * conv_out.astype(jnp.float32)).astype(jnp.bfloat16)
    padded = jnp.pad(dconv.astype(jnp.float32), ((1, 1), (0, 0)))
    grad_u = conv_taps[0] * padded[2:] + conv_taps[1] * padded[1:-1] + conv_taps[2] * padded[:-2]
    grad_c = (grad_u * value_v.astype(jnp.float32)).astype(jnp.bfloat16)
    grad_v = (grad_u * gate_c.astype(jnp.float32)).astype(jnp.bfloat16)
    mixed = (gate_b.astype(jnp.float32) * conv_out.astype(jnp.float32)).astype(jnp.bfloat16)
    grad_out = jnp.dot(grad_h.T, mixed, preferred_element_type=jnp.float32)
    return grad_gate, grad_up, grad_down, grad_out, grad_b, grad_c, grad_v
```

```python
import functools

import jax
import jax.numpy as jnp
from jax import lax
from jax.experimental import pallas as pl
from jax.experimental.pallas import tpu as pltpu
from jax.sharding import PartitionSpec as P

MESH = pl.DeviceIdType.MESH
NX = 4
NY = 4
BF = jnp.bfloat16
F32 = jnp.float32


def block_order(nz):
    order = [0]
    for d in range(1, nz // 2 + 1):
        order.append(d)
        if nz - d != d:
            order.append(nz - d)
    return order[:nz]


class Place:
    def __init__(self, nz):
        self.nz = nz
        self.sp = lax.axis_index("sp")
        self.tp = lax.axis_index("tp")
        self.z = lax.div(self.sp, NX)
        self.x = lax.rem(self.sp, NX)
        self.y = lax.div(self.tp, 2)
        self.c = lax.rem(self.tp, 2)

    def over_sp(self, dz, dx):
        z = lax.rem(self.z + dz, self.nz)
        x = lax.rem(self.x + dx, NX)
        return (z * NX + x, self.tp)

    def over_y(self, dy):
        return (self.sp, lax.rem(self.y + dy + NY, NY) * 2 + self.c)

    def other(self):
        return (self.sp, self.y * 2 + 1 - self.c)

    def origin(self, dy, flip):
        y = lax.rem(self.y + dy + NY, NY)
        c = 1 - self.c if flip else self.c
        return y * 2 + c


def greet(here):
    barrier = pltpu.get_barrier_semaphore()
    peers = [here.over_sp(dz, dx) for dz in range(here.nz) for dx in range(NX) if dz or dx]
    peers += [here.other(), here.over_y(1), here.over_y(-1)]
    for peer in peers:
        pl.semaphore_signal(barrier, inc=1, device_id=peer, device_id_type=MESH)
    return barrier, len(peers)


def send(src, dst, send_sem, recv_sem, peer):
    copy = pltpu.make_async_remote_copy(
        src_ref=src,
        dst_ref=dst,
        send_sem=send_sem,
        recv_sem=recv_sem,
        device_id=peer,
        device_id_type=MESH,
    )
    copy.start()


def await_bytes(ref, sem):
    pltpu.make_async_copy(ref, ref, sem).wait()


class Gather:
    def __init__(self, here, chunk, send_sem, near, far):
        self.here, self.chunk, self.send_sem, self.near, self.far = here, chunk, send_sem, near, far

    def _send(self, origin, h, peer, recv_sem):
        ref = self.chunk(origin, h)
        send(ref, ref, self.send_sem, recv_sem, peer)

    def start(self, h):
        here = self.here
        mine = here.origin(0, False)
        self._send(mine, h, here.over_y(1), self.near.at[0, h])
        self._send(mine, h, here.over_y(-1), self.near.at[1, h])
        self._send(mine, h, here.other(), self.far.at[0])

    def forward(self, h):
        here = self.here
        low, high = here.origin(-1, False), here.origin(1, False)
        await_bytes(self.chunk(low, h), self.near.at[0, h])
        if h % 2 == 0:
            self._send(low, h, here.over_y(1), self.near.at[2, h])
        self._send(low, h, here.other(), self.far.at[1])
        await_bytes(self.chunk(high, h), self.near.at[1, h])
        if h % 2 == 1:
            self._send(high, h, here.over_y(-1), self.near.at[2, h])
        self._send(high, h, here.other(), self.far.at[2])

    def last(self, h):
        here = self.here
        across = here.origin(2, False)
        await_bytes(self.chunk(across, h), self.near.at[2, h])
        self._send(across, h, here.other(), self.far.at[3])

    def finish(self, whole):
        here = self.here
        for k, dy in enumerate((0, -1, 1, 2)):
            await_bytes(whole(here.origin(dy, True)), self.far.at[k])


def slots_of(ids, here, total):
    tokens = ids.shape[0]
    lanes = lax.broadcasted_iota(jnp.int32, (tokens, 128), 1)
    named = [(lanes == ids[:, k : k + 1]).astype(F32) for k in range(2)]
    rows = lax.broadcasted_iota(jnp.int32, (tokens, tokens), 0)
    cols = lax.broadcasted_iota(jnp.int32, (tokens, tokens), 1)
    earlier = (cols < rows).astype(F32).astype(BF)
    before = jnp.dot(earlier, (named[0] + named[1]).astype(BF), preferred_element_type=F32)
    cap = total // (here.nz * NX)
    out = []
    for k in range(2):
        slot = jnp.sum(before * named[k], axis=1, keepdims=True)
        e = ids[:, k : k + 1]
        dz = ((e // NX if NX not in (1, 2, 4) else (e >> (NX.bit_length() - 1))) - here.z) & (here.nz - 1)
        dx = ((e & (NX - 1)) - here.x) & (NX - 1)
        out.append(((dz * NX + dx) * cap).astype(F32) + slot)
    return out


def dispatch_kernel(
    nz, og_ref, x_ref, rw_ref, ids_ref, buf, sbuf, barrier_dummy, own_sem, sp_send, sp_recv, tp_send, near, far
):
    del barrier_dummy
    here = Place(nz)
    barrier, peers = greet(here)
    total, chans = sbuf.shape[1:]
    cap = total // (nz * NX)
    tokens = og_ref.shape[0]

    slots = slots_of(ids_ref[...], here, total)
    srow = lax.broadcasted_iota(jnp.int32, (total, tokens), 0).astype(F32)
    places = []
    for k in range(2):
        wide = jnp.broadcast_to(slots[k], (tokens, tokens)).T
        places.append((srow == wide[0:1, :]).astype(F32))
    both = (places[0] + places[1]).astype(BF)
    sbuf[0] = jnp.dot(both, x_ref[...], preferred_element_type=F32).astype(BF)
    og = og_ref[...].astype(F32)
    dy = None
    for k in range(2):
        weighted = (rw_ref[:, k : k + 1] * og).astype(BF)
        term = jnp.dot(places[k].astype(BF), weighted, preferred_element_type=F32)
        dy = term if dy is None else dy + term
    sbuf[1] = dy.astype(BF)

    order = block_order(nz)
    at = {d: p for p, d in enumerate(order)}
    rows = NX * cap
    column = pl.ds(pl.multiple_of(here.tp * chans, chans), chans)
    pl.semaphore_wait(barrier, peers)
    own = pltpu.make_async_copy(sbuf.at[:, 0:cap, :], buf.at[:, 0:cap, column], own_sem)
    own.start()
    for dz in order:
        for dx in range(NX):
            if dz or dx:
                r = (dz * NX + dx) * cap
                p = at[(-dz) % nz]
                t = p * rows + ((-dx) % NX) * cap
                send(
                    sbuf.at[:, pl.ds(r, cap), :],
                    buf.at[:, pl.ds(t, cap), column],
                    sp_send,
                    sp_recv.at[p],
                    here.over_sp(dz, dx),
                )

    def chunk(origin, h):
        return buf.at[:, pl.ds(h * rows, rows), pl.ds(pl.multiple_of(origin * chans, chans), chans)]

    def whole(origin):
        return buf.at[:, :, pl.ds(pl.multiple_of(origin * chans, chans), chans)]

    gather = Gather(here, chunk, tp_send, near, far)
    for p in range(nz + 2):
        if p < nz:
            if p == 0:
                own.wait()
                await_bytes(buf.at[:, cap:rows, column], sp_recv.at[0])
            else:
                await_bytes(buf.at[:, pl.ds(p * rows, rows), column], sp_recv.at[p])
            gather.start(p)
        if 0 <= p - 1 < nz:
            gather.forward(p - 1)
        if 0 <= p - 2 < nz:
            gather.last(p - 2)
    gather.finish(whole)
    await_bytes(sbuf.at[:, pl.ds(0, total - cap), :], sp_send)
    await_bytes(buf.at[:, pl.ds(0, total - total // (2 * NY)), :], tp_send)


def tail_kernel(
    nz,
    part_ref,
    og_ref,
    ids_ref,
    out_proj_ref,
    conv_ref,
    gb_ref,
    gc_ref,
    vv_ref,
    taps_ref,
    go_ref,
    gradb_ref,
    gradc_ref,
    gradv_ref,
    pr,
    sb,
    ra,
    rb,
    sc,
    rc,
    fin,
    ret,
    dh,
    dhall,
    dht,
    xb,
    xall,
    mixed,
    mx,
    edge,
    halo,
    gpart,
    gr,
    own_sem,
    pair_send,
    pair_recv,
    rs_send,
    rs_recv,
    sp_send,
    sp_recv,
    dh_send,
    dh_near,
    dh_far,
    xb_send,
    xb_near,
    xb_far,
    x_send,
    x_recv,
    m_send,
    m_recv,
    e_send,
    e_recv,
    z_send,
    z_recv,
):
    here = Place(nz)
    barrier, peers = greet(here)
    total = part_ref.shape[0]
    cap = total // (nz * NX)
    rows = NX * cap
    tokens, chans = og_ref.shape
    order = block_order(nz)
    half = total // 2

    slots = slots_of(ids_ref[...], here, total)
    scol = lax.broadcasted_iota(jnp.int32, (tokens, total), 1).astype(F32)
    pick = ((scol == slots[0]).astype(F32) + (scol == slots[1]).astype(F32)).astype(BF)
    mixed[...] = (gb_ref[...].astype(F32) * conv_ref[...].astype(F32)).astype(BF)
    pl.semaphore_wait(barrier, peers)

    for k in (1, 0):
        for y in range(NY):
            col = pl.ds(pl.multiple_of((2 * y + 1 - here.c) * chans, chans), chans)
            send(
                part_ref.at[pl.ds(k * half, half), col],
                pr.at[y, pl.ds(k * half, half), :],
                pair_send,
                pair_recv.at[k],
                here.other(),
            )
    mrow = pl.ds(pl.multiple_of(here.x * tokens, tokens), tokens)
    own_mixed = pltpu.make_async_copy(mixed, mx.at[mrow, :], own_sem.at[0])
    own_mixed.start()
    for dx in range(1, NX):
        send(mixed, mx.at[mrow, :], m_send, m_recv, here.over_sp(0, dx))

    def pair(p, dy):
        y = lax.rem(here.y + dy + NY, NY)
        r = pl.ds(p * rows, rows)
        col = pl.ds(pl.multiple_of((2 * y + here.c) * chans, chans), chans)
        return part_ref[r, col].astype(F32) + pr[y, r, :].astype(F32)

    def stage_a(p):
        way = 1 if p % 2 == 0 else -1
        r = pl.ds(p * rows, rows)
        if p == nz - 1:
            await_bytes(pr.at[:, pl.ds(half, half), :], pair_recv.at[1])
        if p == nz // 2 - 1:
            await_bytes(pr.at[:, pl.ds(0, half), :], pair_recv.at[0])
        sb[0, r, :] = pair(p, 2).astype(BF)
        send(sb.at[0, r, :], ra.at[r, :], rs_send.at[0], rs_recv.at[0, p], here.over_y(way))
        sb[1, r, :] = pair(p, -way).astype(BF)
        send(sb.at[1, r, :], rb.at[r, :], rs_send.at[1], rs_recv.at[1, p], here.over_y(-way))

    def stage_b(p):
        way = 1 if p % 2 == 0 else -1
        r = pl.ds(p * rows, rows)
        await_bytes(ra.at[r, :], rs_recv.at[0, p])
        sc[r, :] = (pair(p, way) + ra[r, :].astype(F32)).astype(BF)
        send(sc.at[r, :], rc.at[r, :], rs_send.at[2], rs_recv.at[2, p], here.over_y(way))

    def stage_c(p):
        r = pl.ds(p * rows, rows)
        await_bytes(rb.at[r, :], rs_recv.at[1, p])
        await_bytes(rc.at[r, :], rs_recv.at[2, p])
        fin[r, :] = (pair(p, 0) + rb[r, :].astype(F32) + rc[r, :].astype(F32)).astype(BF)
        dz = order[p]
        for dx in range(NX):
            src = fin.at[pl.ds(p * rows + dx * cap, cap), :]
            t = (((-dz) % nz) * NX + (-dx) % NX) * cap
            dst = ret.at[pl.ds(t, cap), :]
            if dz or dx:
                send(src, dst, sp_send, sp_recv, here.over_sp(dz, dx))

    for s in range(nz + 2):
        if s < nz:
            stage_a(nz - 1 - s)
        if 0 <= s - 1 < nz:
            stage_b(nz - s)
        if 0 <= s - 2 < nz:
            stage_c(nz + 1 - s)
    ret[0:cap, :] = fin[0:cap, :]
    await_bytes(ret.at[pl.ds(cap, total - cap), :], sp_recv)

    moe = jnp.dot(pick, ret[...], preferred_element_type=F32)
    grad_h = og_ref[...].astype(F32) + moe
    dht[...] = grad_h.T.astype(BF)
    dh[...] = grad_h.astype(BF)

    wide = chans // NX
    tcol = pl.ds(pl.multiple_of(here.x * tokens, tokens), tokens)
    block = pl.ds(pl.multiple_of(here.tp * wide, wide), wide)
    for dx in range(1, NX):
        to = lax.rem(here.x + dx, NX)
        send(
            dht.at[pl.ds(pl.multiple_of(to * wide, wide), wide), :],
            xb.at[:, tcol],
            x_send,
            x_recv,
            here.over_sp(0, dx),
        )
    own_x = pltpu.make_async_copy(
        dht.at[pl.ds(pl.multiple_of(here.x * wide, wide), wide), :], xb.at[:, tcol], own_sem.at[1]
    )
    own_x.start()
    hcol = pl.ds(pl.multiple_of(here.tp * chans, chans), chans)
    own_dh = pltpu.make_async_copy(dh, dhall.at[:, hcol], own_sem.at[2])
    own_dh.start()
    own_dh.wait()

    def dh_chunk(origin, h):
        return dhall.at[
            pl.ds(h * (tokens // 2), tokens // 2), pl.ds(pl.multiple_of(origin * chans, chans), chans)
        ]

    def dh_whole(origin):
        return dhall.at[:, pl.ds(pl.multiple_of(origin * chans, chans), chans)]

    def xb_chunk(origin, h):
        return xall.at[pl.ds(pl.multiple_of(origin * wide + h * (wide // 2), wide // 2), wide // 2), :]

    def xb_whole(origin):
        return xall.at[pl.ds(pl.multiple_of(origin * wide, wide), wide), :]

    dh_gather = Gather(here, dh_chunk, dh_send, dh_near, dh_far)
    xb_gather = Gather(here, xb_chunk, xb_send, xb_near, xb_far)
    dh_gather.start(0)
    dh_gather.start(1)
    own_x.wait()
    await_bytes(xb.at[:, pl.ds(0, (NX - 1) * tokens)], x_recv)
    place_x = pltpu.make_async_copy(xb, xall.at[block, :], own_sem.at[3])
    place_x.start()
    place_x.wait()
    xb_gather.start(0)
    xb_gather.start(1)
    for h in range(2):
        dh_gather.forward(h)
    for h in range(2):
        xb_gather.forward(h)
    for h in range(2):
        dh_gather.last(h)
    for h in range(2):
        xb_gather.last(h)
    dh_gather.finish(dh_whole)
    grad_z = jnp.dot(dhall[...], out_proj_ref[...], preferred_element_type=F32)
    dconv = (grad_z * gb_ref[...].astype(F32)).astype(BF)
    edge[0, :, :] = dconv[0:16, :]
    edge[1, :, :] = dconv[tokens - 16 :, :]
    last_sp = nz * NX
    before = (lax.rem(here.sp + last_sp - 1, last_sp), here.tp)
    after = (lax.rem(here.sp + 1, last_sp), here.tp)
    send(edge.at[0], halo.at[1], e_send.at[0], e_recv.at[1], before)
    send(edge.at[1], halo.at[0], e_send.at[1], e_recv.at[0], after)
    gradb_ref[...] = (grad_z * conv_ref[...].astype(F32)).astype(BF)

    own_mixed.wait()
    await_bytes(mx.at[pl.ds(0, (NX - 1) * tokens), :], m_recv)
    xb_gather.finish(xb_whole)
    gpart[...] = jnp.dot(xall[...], mx[...], preferred_element_type=F32).astype(BF)
    for dz in range(1, nz):
        to = lax.rem(here.z + dz, nz)
        send(
            gpart.at[pl.ds(pl.multiple_of(to * wide, wide), wide), :],
            gr.at[dz],
            z_send,
            z_recv,
            here.over_sp(dz, 0),
        )
    own_g = pltpu.make_async_copy(
        gpart.at[pl.ds(pl.multiple_of(here.z * wide, wide), wide), :], gr.at[0], own_sem.at[4]
    )
    own_g.start()

    await_bytes(halo.at[0], e_recv.at[0])
    await_bytes(halo.at[1], e_recv.at[1])
    dconv = dconv.astype(F32)
    row = lax.broadcasted_iota(jnp.int32, dconv.shape, 0)
    low = halo[0].astype(F32)[15:16, :] * (here.sp > 0).astype(F32)
    high = halo[1].astype(F32)[0:1, :] * (here.sp < last_sp - 1).astype(F32)
    prev = jnp.where(row == 0, low, pltpu.roll(dconv, 1, 0))
    nxt = jnp.where(row == tokens - 1, high, pltpu.roll(dconv, tokens - 1, 0))
    grad_u = taps_ref[0:1, :] * nxt + taps_ref[1:2, :] * dconv + taps_ref[2:3, :] * prev
    gradc_ref[...] = (grad_u * vv_ref[...].astype(F32)).astype(BF)
    gradv_ref[...] = (grad_u * gc_ref[...].astype(F32)).astype(BF)

    own_g.wait()
    await_bytes(gr.at[pl.ds(1, nz - 1)], z_recv)
    summed = gr[0].astype(F32)
    for k in range(1, nz):
        summed = summed + gr[k].astype(F32)
    go_ref[...] = summed

    await_bytes(pr, pair_send)
    for k in range(3):
        await_bytes(ra, rs_send.at[k])
    await_bytes(ret.at[pl.ds(cap, total - cap), :], sp_send)
    await_bytes(dhall.at[:, pl.ds(0, (2 * NY - 1) * chans)], dh_send)
    await_bytes(xall.at[pl.ds(0, (2 * NY - 1) * wide), :], xb_send)
    await_bytes(xb.at[:, pl.ds(0, (NX - 1) * tokens)], x_send)
    await_bytes(mx.at[pl.ds(0, (NX - 1) * tokens), :], m_send)
    await_bytes(edge.at[0], e_send.at[0])
    await_bytes(edge.at[1], e_send.at[1])
    await_bytes(gr.at[pl.ds(1, nz - 1)], z_send)


VM = pl.BlockSpec(memory_space=pltpu.VMEM)


def local(
    nz,
    ntp,
    out_grad,
    moe_input,
    route_weight,
    route_ids,
    gate_proj,
    up_proj,
    down_proj,
    out_proj,
    conv_out,
    gate_b,
    gate_c,
    value_v,
    conv_taps,
):
    tokens, chans = out_grad.shape
    ns = nz * NX
    cap = 4 * tokens // ns
    total = ns * cap
    width = chans * ntp
    dma = pltpu.SemaphoreType.DMA
    buf = pl.pallas_call(
        functools.partial(dispatch_kernel, nz),
        out_shape=jax.ShapeDtypeStruct((2, total, width), BF),
        in_specs=[VM] * 4,
        out_specs=VM,
        scratch_shapes=[
            pltpu.VMEM((2, total, chans), BF),
            pltpu.VMEM((8, 128), F32),
            dma,
            dma,
            dma((nz,)),
            dma,
            dma((3, nz)),
            dma((4,)),
        ],
        compiler_params=pltpu.CompilerParams(collective_id=0, has_side_effects=True),
        name="dispatch",
    )(out_grad, moe_input, route_weight, route_ids)
    xin, dyin = buf[0], buf[1]
    w_gate, w_up, w_down = gate_proj[0], up_proj[0], down_proj[0]
    gate = jnp.dot(xin, w_gate, preferred_element_type=F32)
    upval = jnp.dot(xin, w_up, preferred_element_type=F32)
    sig = jax.nn.sigmoid(gate)
    act = gate * sig
    hidden = (act * upval).astype(BF)
    dhid = jnp.dot(dyin, w_down.T, preferred_element_type=F32)
    dgate = (dhid * upval * (sig * (1.0 + gate * (1.0 - sig)))).astype(BF)
    dup = (dhid * act).astype(BF)
    part = (
        jnp.dot(dgate, w_gate.T, preferred_element_type=F32)
        + jnp.dot(dup, w_up.T, preferred_element_type=F32)
    ).astype(BF)
    grad_down = jnp.dot(hidden.T, dyin, preferred_element_type=F32).astype(BF)
    grad_gate = jnp.dot(xin.T, dgate, preferred_element_type=F32).astype(BF)
    grad_up = jnp.dot(xin.T, dup, preferred_element_type=F32).astype(BF)

    wide = chans // NX
    vm = pltpu.VMEM
    grad_out, grad_b, grad_c, grad_v = pl.pallas_call(
        functools.partial(tail_kernel, nz),
        out_shape=[
            jax.ShapeDtypeStruct((wide, chans), F32),
            jax.ShapeDtypeStruct((tokens, chans), BF),
            jax.ShapeDtypeStruct((tokens, chans), BF),
            jax.ShapeDtypeStruct((tokens, chans), BF),
        ],
        in_specs=[VM] * 9,
        out_specs=[VM] * 4,
        scratch_shapes=[
            vm((NY, total, chans), BF),
            vm((2, total, chans), BF),
            vm((total, chans), BF),
            vm((total, chans), BF),
            vm((total, chans), BF),
            vm((total, chans), BF),
            vm((total, chans), BF),
            vm((total, chans), BF),
            vm((tokens, chans), BF),
            vm((tokens, width), BF),
            vm((chans, tokens), BF),
            vm((wide, NX * tokens), BF),
            vm((ntp * wide, NX * tokens), BF),
            vm((tokens, chans), BF),
            vm((NX * tokens, chans), BF),
            vm((2, 16, chans), BF),
            vm((2, 16, chans), BF),
            vm((nz * wide, chans), BF),
            vm((nz, wide, chans), BF),
            dma((5,)),
            dma,
            dma((2,)),
            dma((3,)),
            dma((3, nz)),
            dma,
            dma,
            dma,
            dma((3, 2)),
            dma((4,)),
            dma,
            dma((3, 2)),
            dma((4,)),
            dma,
            dma,
            dma,
            dma,
            dma((2,)),
            dma((2,)),
            dma,
            dma,
        ],
        compiler_params=pltpu.CompilerParams(collective_id=1, has_side_effects=True),
        name="tail",
    )(part, out_grad, route_ids, out_proj, conv_out, gate_b, gate_c, value_v, conv_taps)
    return (grad_gate[None], grad_up[None], grad_down[None], grad_out, grad_b, grad_c, grad_v)


def solution(mesh):
    nz = mesh.shape["sp"] // NX
    ntp = mesh.shape["tp"]
    tok, tok_tp = P("sp", None), P("sp", "tp")
    return jax.shard_map(
        functools.partial(local, nz, ntp),
        mesh=mesh,
        in_specs=(
            tok_tp,
            tok_tp,
            tok,
            tok,
            P("sp", None, "tp"),
            P("sp", None, "tp"),
            P("sp", "tp", None),
            P(None, "tp"),
            tok_tp,
            tok_tp,
            tok_tp,
            tok_tp,
            P(None, "tp"),
        ),
        out_specs=(
            P("sp", None, "tp"),
            P("sp", None, "tp"),
            P("sp", "tp", None),
            tok_tp,
            tok_tp,
            tok_tp,
            tok_tp,
        ),
        check_vma=False,
    )
```

```python
import functools

import jax
import jax.numpy as jnp
from jax import lax
from jax.experimental import pallas as pl
from jax.experimental.pallas import tpu as pltpu
from jax.sharding import PartitionSpec as P

MESH = pl.DeviceIdType.MESH
NX = 4
NY = 4
BF = jnp.bfloat16
F32 = jnp.float32


def block_order(nz):
    order = [0]
    for d in range(1, nz // 2 + 1):
        order.append(d)
        if nz - d != d:
            order.append(nz - d)
    return order[:nz]


class Place:
    def __init__(self, nz):
        self.nz = nz
        self.sp = lax.axis_index("sp")
        self.tp = lax.axis_index("tp")
        self.z = lax.div(self.sp, NX)
        self.x = lax.rem(self.sp, NX)
        self.y = lax.div(self.tp, 2)
        self.c = lax.rem(self.tp, 2)

    def over_sp(self, dz, dx):
        z = lax.rem(self.z + dz, self.nz)
        x = lax.rem(self.x + dx, NX)
        return (z * NX + x, self.tp)

    def over_y(self, dy):
        return (self.sp, lax.rem(self.y + dy + NY, NY) * 2 + self.c)

    def other(self):
        return (self.sp, self.y * 2 + 1 - self.c)

    def origin(self, dy, flip):
        y = lax.rem(self.y + dy + NY, NY)
        c = 1 - self.c if flip else self.c
        return y * 2 + c


def greet(here):
    barrier = pltpu.get_barrier_semaphore()
    peers = [here.over_sp(dz, dx) for dz in range(here.nz) for dx in range(NX) if dz or dx]
    peers += [here.other(), here.over_y(1), here.over_y(-1)]
    for peer in peers:
        pl.semaphore_signal(barrier, inc=1, device_id=peer, device_id_type=MESH)
    return barrier, len(peers)


def send(src, dst, send_sem, recv_sem, peer):
    copy = pltpu.make_async_remote_copy(
        src_ref=src,
        dst_ref=dst,
        send_sem=send_sem,
        recv_sem=recv_sem,
        device_id=peer,
        device_id_type=MESH,
    )
    copy.start()


def await_bytes(ref, sem):
    pltpu.make_async_copy(ref, ref, sem).wait()


class Gather:
    def __init__(self, here, chunk, send_sem, near, far, group=lambda h: 0):
        self.here, self.chunk, self.send_sem = here, chunk, send_sem
        self.near, self.far, self.group = near, far, group

    def _send(self, origin, h, peer, recv_sem):
        ref = self.chunk(origin, h)
        send(ref, ref, self.send_sem, recv_sem, peer)

    def start(self, h):
        here = self.here
        mine = here.origin(0, False)
        self._send(mine, h, here.over_y(1), self.near.at[0, h])
        self._send(mine, h, here.over_y(-1), self.near.at[1, h])
        self._send(mine, h, here.other(), self.far.at[0, self.group(h)])

    def forward(self, h):
        here = self.here
        low, high = here.origin(-1, False), here.origin(1, False)
        await_bytes(self.chunk(low, h), self.near.at[0, h])
        if h % 2 == 0:
            self._send(low, h, here.over_y(1), self.near.at[2, h])
        self._send(low, h, here.other(), self.far.at[1, self.group(h)])
        await_bytes(self.chunk(high, h), self.near.at[1, h])
        if h % 2 == 1:
            self._send(high, h, here.over_y(-1), self.near.at[2, h])
        self._send(high, h, here.other(), self.far.at[2, self.group(h)])

    def last(self, h):
        here = self.here
        across = here.origin(2, False)
        await_bytes(self.chunk(across, h), self.near.at[2, h])
        self._send(across, h, here.other(), self.far.at[3, self.group(h)])

    def finish(self, whole, g=0):
        here = self.here
        for k, dy in enumerate((0, -1, 1, 2)):
            await_bytes(whole(here.origin(dy, True)), self.far.at[k, g])


def slots_of(ids, here, total):
    tokens = ids.shape[0]
    lanes = lax.broadcasted_iota(jnp.int32, (tokens, 128), 1)
    named = [(lanes == ids[:, k : k + 1]).astype(F32) for k in range(2)]
    rows = lax.broadcasted_iota(jnp.int32, (tokens, tokens), 0)
    cols = lax.broadcasted_iota(jnp.int32, (tokens, tokens), 1)
    earlier = (cols < rows).astype(F32).astype(BF)
    before = jnp.dot(earlier, (named[0] + named[1]).astype(BF), preferred_element_type=F32)
    cap = total // (here.nz * NX)
    out = []
    for k in range(2):
        slot = jnp.sum(before * named[k], axis=1, keepdims=True)
        e = ids[:, k : k + 1]
        dz = ((e // NX if NX not in (1, 2, 4) else (e >> (NX.bit_length() - 1))) - here.z) & (here.nz - 1)
        dx = ((e & (NX - 1)) - here.x) & (NX - 1)
        out.append(((dz * NX + dx) * cap).astype(F32) + slot)
    return out


def nt(a, b):
    return lax.dot_general(a, b, (((1,), (1,)), ((), ())), preferred_element_type=F32)


def step_kernel(
    nz,
    og_ref,
    x_ref,
    rw_ref,
    ids_ref,
    conv_ref,
    gb_ref,
    gc_ref,
    vv_ref,
    taps_ref,
    wg_hbm,
    wu_hbm,
    wd_hbm,
    op_hbm,
    go_ref,
    gradb_ref,
    gradc_ref,
    gradv_ref,
    rows_hbm,
    dt_hbm,
    sbuf,
    buf,
    wcat,
    wd,
    out_proj,
    dcat,
    dt,
    part,
    pr,
    sb,
    ra,
    rb,
    sc,
    rc,
    fin,
    ret,
    pick,
    dh,
    dhall,
    dht,
    xall,
    mixed,
    mx,
    edge,
    halo,
    gpart,
    gr,
    w_sem,
    own_sem,
    a_send,
    a_recv,
    g_send,
    g_near,
    g_far,
    pair_send,
    pair_recv,
    rs_send,
    rs_recv,
    sp_send,
    sp_recv,
    dh_send,
    dh_near,
    dh_far,
    xb_send,
    xb_near,
    xb_far,
    x_send,
    x_recv,
    m_send,
    m_recv,
    e_send,
    e_recv,
    z_send,
    z_recv,
):
    here = Place(nz)
    barrier, peers = greet(here)
    total, chans = sbuf.shape[1:]
    cap = total // (nz * NX)
    tokens = og_ref.shape[0]
    hid, padded = wg_hbm.shape[0], wd.shape[0]
    order = block_order(nz)
    at = {d: p for p, d in enumerate(order)}
    rows = NX * cap
    half = total // 2
    hb = nz // 2

    loads = [
        pltpu.make_async_copy(wg_hbm, wcat.at[0:hid, :], w_sem.at[0]),
        pltpu.make_async_copy(wu_hbm, wcat.at[padded : padded + hid, :], w_sem.at[1]),
        pltpu.make_async_copy(wd_hbm, wd.at[0:hid, :], w_sem.at[2]),
        pltpu.make_async_copy(op_hbm, out_proj, w_sem.at[3]),
    ]
    for load in loads:
        load.start()

    ids = ids_ref[...].astype(F32).T.astype(jnp.int32)
    rw = rw_ref[...].T
    slots = slots_of(ids, here, total)
    srow = lax.broadcasted_iota(jnp.int32, (total, tokens), 0).astype(F32)
    places = []
    for k in range(2):
        wide = jnp.broadcast_to(slots[k], (tokens, tokens)).T
        places.append((srow == wide[0:1, :]).astype(F32))
    both = (places[0] + places[1]).astype(BF)
    sbuf[0] = jnp.dot(both, x_ref[...], preferred_element_type=F32).astype(BF)
    og = og_ref[...].astype(F32)
    dy = None
    for k in range(2):
        weighted = (rw[:, k : k + 1] * og).astype(BF)
        term = jnp.dot(places[k].astype(BF), weighted, preferred_element_type=F32)
        dy = term if dy is None else dy + term
    sbuf[1] = dy.astype(BF)
    scol = lax.broadcasted_iota(jnp.int32, (tokens, total), 1).astype(F32)
    pick[...] = ((scol == slots[0]).astype(F32) + (scol == slots[1]).astype(F32)).astype(BF)
    mixed[...] = (gb_ref[...].astype(F32) * conv_ref[...].astype(F32)).astype(BF)
    wcat[hid:padded, :] = jnp.zeros((padded - hid, wcat.shape[1]), BF)
    wcat[padded + hid :, :] = jnp.zeros((padded - hid, wcat.shape[1]), BF)
    wd[hid:, :] = jnp.zeros((padded - hid, wcat.shape[1]), BF)

    def cols(origin):
        return pl.ds(pl.multiple_of(origin * chans, chans), chans)

    column = cols(here.tp)
    pl.semaphore_wait(barrier, peers)
    own = pltpu.make_async_copy(sbuf.at[:, 0:cap, :], buf.at[:, 0:cap, column], own_sem.at[5])
    own.start()
    for dz in order:
        for dx in range(NX):
            if dz or dx:
                r = (dz * NX + dx) * cap
                p = at[(-dz) % nz]
                t = p * rows + ((-dx) % NX) * cap
                send(
                    sbuf.at[:, pl.ds(r, cap), :],
                    buf.at[:, pl.ds(t, cap), column],
                    a_send,
                    a_recv.at[p],
                    here.over_sp(dz, dx),
                )
    mrow = pl.ds(pl.multiple_of(here.x * tokens, tokens), tokens)
    own_mixed = pltpu.make_async_copy(mixed, mx.at[mrow, :], own_sem.at[0])
    own_mixed.start()

    def chunk(origin, h):
        return buf.at[:, pl.ds(h * rows, rows), cols(origin)]

    gather = Gather(here, chunk, g_send, g_near, g_far, lambda h: h // hb)

    def experts(r0, n):
        r = pl.ds(r0, n)
        gu = nt(buf[0, r, :], wcat[...])
        dhid = nt(buf[1, r, :], wd[...])
        gate, upval = gu[:, :padded], gu[:, padded:]
        sig = jax.nn.sigmoid(gate)
        act = gate * sig
        dcat[r, 0:padded] = (dhid * upval * (sig * (1.0 + gate * (1.0 - sig)))).astype(BF)
        dcat[r, padded : 2 * padded] = (dhid * act).astype(BF)
        dcat[r, 2 * padded :] = (act * upval).astype(BF)

    def whole(k):
        return lambda origin: buf.at[:, pl.ds(k * half, half), cols(origin)]

    def early(step):
        if step == 0:
            gather.finish(whole(0), 0)
            for load in loads[:3]:
                load.wait()
        n = half // EARLY
        if step < EARLY:
            experts(step * n, n)

    done = 0
    for p in range(nz + LAST):
        if p < nz:
            if p == 0:
                own.wait()
                await_bytes(buf.at[:, cap:rows, column], a_recv.at[0])
            else:
                await_bytes(buf.at[:, pl.ds(p * rows, rows), column], a_recv.at[p])
            gather.start(p)
        if p == nz - 1:
            for dx in range(1, NX):
                send(mixed, mx.at[mrow, :], m_send, m_recv, here.over_sp(0, dx))
        if 0 <= p - FORWARD < nz:
            gather.forward(p - FORWARD)
        if 0 <= p - LAST < nz:
            gather.last(p - LAST)
        if p >= hb + LAST and done < EARLY:
            early(done)
            done += 1
    while done < EARLY:
        early(done)
        done += 1
    gather.finish(whole(1), 1)
    keep_rows = pltpu.make_async_copy(buf, rows_hbm, own_sem.at[6])
    keep_rows.start()
    experts(half, half)

    def spread(k):
        r = pl.ds(k * half, half)
        d = dcat[r, 0 : 2 * padded]
        step = 2 * chans
        for n in range(NY):
            c = pl.ds(n * step, step)
            part[r, c] = jnp.dot(d, wcat[:, c], preferred_element_type=F32).astype(BF)
        for y in range(NY):
            send(
                part.at[r, cols(2 * y + 1 - here.c)],
                pr.at[y, r, :],
                pair_send,
                pair_recv.at[k],
                here.other(),
            )

    spread(1)
    spread(0)

    def pair(p, dy):
        y = lax.rem(here.y + dy + NY, NY)
        r = pl.ds(p * rows, rows)
        return part[r, cols(2 * y + here.c)].astype(F32) + pr[y, r, :].astype(F32)

    def stage_a(p):
        way = 1 if p % 2 == 0 else -1
        r = pl.ds(p * rows, rows)
        if p == nz - 1:
            await_bytes(pr.at[:, pl.ds(half, half), :], pair_recv.at[1])
        if p == hb - 1:
            await_bytes(pr.at[:, pl.ds(0, half), :], pair_recv.at[0])
        sb[0, r, :] = pair(p, 2).astype(BF)
        send(sb.at[0, r, :], ra.at[r, :], rs_send.at[0], rs_recv.at[0, p], here.over_y(way))
        sb[1, r, :] = pair(p, -way).astype(BF)
        send(sb.at[1, r, :], rb.at[r, :], rs_send.at[1], rs_recv.at[1, p], here.over_y(-way))

    def stage_b(p):
        way = 1 if p % 2 == 0 else -1
        r = pl.ds(p * rows, rows)
        await_bytes(ra.at[r, :], rs_recv.at[0, p])
        sc[r, :] = (pair(p, way) + ra[r, :].astype(F32)).astype(BF)
        send(sc.at[r, :], rc.at[r, :], rs_send.at[2], rs_recv.at[2, p], here.over_y(way))

    def stage_c(p):
        r = pl.ds(p * rows, rows)
        await_bytes(rb.at[r, :], rs_recv.at[1, p])
        await_bytes(rc.at[r, :], rs_recv.at[2, p])
        fin[r, :] = (pair(p, 0) + rb[r, :].astype(F32) + rc[r, :].astype(F32)).astype(BF)
        dz = order[p]
        for dx in range(NX):
            src = fin.at[pl.ds(p * rows + dx * cap, cap), :]
            t = (((-dz) % nz) * NX + (-dx) % NX) * cap
            dst = ret.at[pl.ds(t, cap), :]
            if dz or dx:
                send(src, dst, sp_send, sp_recv, here.over_sp(dz, dx))

    for s in range(nz + STAGE_C):
        if s < nz:
            stage_a(nz - 1 - s)
        if 0 <= s - STAGE_B < nz:
            stage_b(nz - 1 - (s - STAGE_B))
        if 0 <= s - STAGE_C < nz:
            stage_c(nz - 1 - (s - STAGE_C))
    ret[0:cap, :] = fin[0:cap, :]

    slab = 3 * padded // 9

    def turn(k):
        dt[k * slab : (k + 1) * slab, :] = dcat[:, k * slab : (k + 1) * slab].astype(F32).T.astype(BF)

    for k in range(3):
        turn(k)
    await_bytes(ret.at[pl.ds(cap, total - cap), :], sp_recv)

    moe = jnp.dot(pick[...], ret[...], preferred_element_type=F32)
    grad_h = og_ref[...].astype(F32) + moe
    dht[...] = grad_h.T.astype(BF)
    dh[...] = grad_h.astype(BF)

    wide = chans // NX
    tcol = pl.ds(pl.multiple_of(here.x * tokens, tokens), tokens)

    def orows(origin, h=0, n=1):
        size = wide // n
        return pl.ds(pl.multiple_of(origin * wide + h * size, size), size)

    for dx in range(1, NX):
        to = lax.rem(here.x + dx, NX)
        send(
            dht.at[orows(to), :],
            xall.at[orows(here.tp), tcol],
            x_send,
            x_recv,
            here.over_sp(0, dx),
        )
    own_x = pltpu.make_async_copy(dht.at[orows(here.x), :], xall.at[orows(here.tp), tcol], own_sem.at[1])
    own_x.start()
    own_dh = pltpu.make_async_copy(dh, dhall.at[:, column], own_sem.at[2])
    own_dh.start()
    own_dh.wait()
    ht = tokens // 2
    dh_gather = Gather(here, lambda o, h: dhall.at[pl.ds(h * ht, ht), cols(o)], dh_send, dh_near, dh_far)
    xb_gather = Gather(here, lambda o, h: xall.at[orows(o, h, 2), :], xb_send, xb_near, xb_far)
    dh_gather.start(0)
    dh_gather.start(1)
    for k in range(3, 6):
        turn(k)
    own_x.wait()
    await_bytes(xall.at[pl.ds(0, wide), pl.ds(0, (NX - 1) * tokens)], x_recv)
    xb_gather.start(0)
    xb_gather.start(1)
    for h in range(2):
        dh_gather.forward(h)
    for h in range(2):
        dh_gather.last(h)
    for k in range(6, 9):
        turn(k)
    keep_dt = pltpu.make_async_copy(dt, dt_hbm, own_sem.at[3])
    keep_dt.start()
    for h in range(2):
        xb_gather.forward(h)
    dh_gather.finish(lambda o: dhall.at[:, cols(o)])
    loads[3].wait()
    grad_z = jnp.dot(dhall[...], out_proj[...], preferred_element_type=F32)
    dconv = (grad_z * gb_ref[...].astype(F32)).astype(BF)
    edge[0, :, :] = dconv[0:16, :]
    edge[1, :, :] = dconv[tokens - 16 :, :]
    last_sp = nz * NX
    before = (lax.rem(here.sp + last_sp - 1, last_sp), here.tp)
    after = (lax.rem(here.sp + 1, last_sp), here.tp)
    for h in range(2):
        xb_gather.last(h)
    send(edge.at[0], halo.at[1], e_send.at[0], e_recv.at[1], before)
    send(edge.at[1], halo.at[0], e_send.at[1], e_recv.at[0], after)
    own_mixed.wait()
    await_bytes(mx.at[pl.ds(0, (NX - 1) * tokens), :], m_recv)
    xb_gather.finish(lambda o: xall.at[orows(o), :])
    gpart[...] = jnp.dot(xall[...], mx[...], preferred_element_type=F32).astype(BF)
    for dz in range(1, nz):
        to = lax.rem(here.z + dz, nz)
        send(gpart.at[orows(to), :], gr.at[dz], z_send, z_recv, here.over_sp(dz, 0))
    own_g = pltpu.make_async_copy(gpart.at[orows(here.z), :], gr.at[0], own_sem.at[4])
    own_g.start()

    gradb_ref[...] = (grad_z * conv_ref[...].astype(F32)).astype(BF)
    await_bytes(halo.at[0], e_recv.at[0])
    await_bytes(halo.at[1], e_recv.at[1])
    dconv = dconv.astype(F32)
    row = lax.broadcasted_iota(jnp.int32, dconv.shape, 0)
    low = halo[0].astype(F32)[15:16, :] * (here.sp > 0).astype(F32)
    high = halo[1].astype(F32)[0:1, :] * (here.sp < last_sp - 1).astype(F32)
    prev = jnp.where(row == 0, low, pltpu.roll(dconv, 1, 0))
    nxt = jnp.where(row == tokens - 1, high, pltpu.roll(dconv, tokens - 1, 0))
    grad_u = taps_ref[0:1, :] * nxt + taps_ref[1:2, :] * dconv + taps_ref[2:3, :] * prev
    gradc_ref[...] = (grad_u * vv_ref[...].astype(F32)).astype(BF)
    gradv_ref[...] = (grad_u * gc_ref[...].astype(F32)).astype(BF)

    others = 2 * NY - 1
    await_bytes(sbuf.at[:, pl.ds(0, total - cap), :], a_send)
    await_bytes(buf.at[:, pl.ds(0, total - total // (2 * NY)), :], g_send)
    await_bytes(pr, pair_send)
    for k in range(3):
        await_bytes(ra, rs_send.at[k])
    await_bytes(ret.at[pl.ds(cap, total - cap), :], sp_send)
    await_bytes(dhall.at[:, pl.ds(0, others * chans)], dh_send)
    await_bytes(xall.at[pl.ds(0, others * wide), :], xb_send)
    await_bytes(xall.at[pl.ds(0, wide), pl.ds(0, (NX - 1) * tokens)], x_send)
    await_bytes(mx.at[pl.ds(0, (NX - 1) * tokens), :], m_send)
    await_bytes(edge.at[0], e_send.at[0])
    await_bytes(edge.at[1], e_send.at[1])
    keep_rows.wait()
    keep_dt.wait()

    own_g.wait()
    await_bytes(gr.at[pl.ds(1, nz - 1)], z_recv)
    summed = gr[0].astype(F32)
    for k in range(1, nz):
        summed = summed + gr[k].astype(F32)
    go_ref[...] = summed
    await_bytes(gr.at[pl.ds(1, nz - 1)], z_send)


def grads_kernel(rows_ref, dt_ref, go, gb, gc, gv, gate_ref, up_ref, down_ref, go_ref, gb_ref, gc_ref, gv_ref):
    hid, padded = gate_ref.shape[0], dt_ref.shape[0] // 3
    x, dy = rows_ref[0], rows_ref[1]
    both = jnp.dot(dt_ref[0 : 2 * padded, :], x, preferred_element_type=F32)
    gate_ref[...] = both[0:hid, :].astype(BF)
    up_ref[...] = both[padded : padded + hid, :].astype(BF)
    down_ref[...] = jnp.dot(dt_ref[2 * padded :, :], dy, preferred_element_type=F32)[0:hid, :].astype(BF)

    @pl.when(pl.program_id(0) == 0)
    def _():
        go_ref[...] = go[...]
        gb_ref[...] = gb[...]
        gc_ref[...] = gc[...]
        gv_ref[...] = gv[...]


VM = pl.BlockSpec(memory_space=pltpu.VMEM)
ANY = pl.BlockSpec(memory_space=pl.ANY)
FORWARD, LAST = 2, 4
STAGE_B, STAGE_C = 2, 4
EARLY = 2


def local(
    nz,
    ntp,
    out_grad,
    moe_input,
    route_weight,
    route_ids,
    gate_proj,
    up_proj,
    down_proj,
    out_proj,
    conv_out,
    gate_b,
    gate_c,
    value_v,
    conv_taps,
):
    tokens, chans = out_grad.shape
    ns = nz * NX
    cap = 4 * tokens // ns
    total = ns * cap
    width = chans * ntp
    hid = gate_proj.shape[2]
    padded = -(-hid // 128) * 128
    wide = chans // NX
    dma = pltpu.SemaphoreType.DMA

    def vm(*shape):
        return pltpu.VMEM(shape, BF)

    small = [
        jax.ShapeDtypeStruct((wide, chans), F32),
        jax.ShapeDtypeStruct((tokens, chans), BF),
        jax.ShapeDtypeStruct((tokens, chans), BF),
        jax.ShapeDtypeStruct((tokens, chans), BF),
    ]
    *results, kept_rows, kept_dt = pl.pallas_call(
        functools.partial(step_kernel, nz),
        out_shape=[
            *small,
            jax.ShapeDtypeStruct((2, total, width), BF),
            jax.ShapeDtypeStruct((3 * padded, total), BF),
        ],
        in_specs=[VM] * 9 + [ANY] * 4,
        out_specs=[VM] * 4 + [ANY] * 2,
        scratch_shapes=[
            vm(2, total, chans),
            vm(2, total, width),
            vm(2 * padded, width),
            vm(padded, width),
            vm(width, chans),
            vm(total, 3 * padded),
            vm(3 * padded, total),
            vm(total, width),
            vm(NY, total, chans),
            vm(2, total, chans),
            vm(total, chans),
            vm(total, chans),
            vm(total, chans),
            vm(total, chans),
            vm(total, chans),
            vm(total, chans),
            vm(tokens, total),
            vm(tokens, chans),
            vm(tokens, width),
            vm(chans, tokens),
            vm(ntp * wide, NX * tokens),
            vm(tokens, chans),
            vm(NX * tokens, chans),
            vm(2, 16, chans),
            vm(2, 16, chans),
            vm(nz * wide, chans),
            vm(nz, wide, chans),
            dma((4,)),
            dma((7,)),
            dma,
            dma((nz,)),
            dma,
            dma((3, nz)),
            dma((4, 2)),
            dma,
            dma((2,)),
            dma((3,)),
            dma((3, nz)),
            dma,
            dma,
            dma,
            dma((3, 2)),
            dma((4, 1)),
            dma,
            dma((3, 2)),
            dma((4, 1)),
            dma,
            dma,
            dma,
            dma,
            dma((2,)),
            dma((2,)),
            dma,
            dma,
        ],
        compiler_params=pltpu.CompilerParams(
            collective_id=0, has_side_effects=True, vmem_limit_bytes=60 * 1024 * 1024
        ),
        name="step",
    )(
        out_grad,
        moe_input,
        route_weight.T,
        route_ids.T,
        conv_out,
        gate_b,
        gate_c,
        value_v,
        conv_taps,
        gate_proj[0].T,
        up_proj[0].T,
        down_proj[0],
        out_proj,
    )

    step = width // 8

    def held(shape):
        return pl.BlockSpec(shape, lambda i: (0, 0))

    weights = pl.BlockSpec((hid, step), lambda i: (0, i))
    grad_gate, grad_up, grad_down, grad_out, grad_b, grad_c, grad_v = pl.pallas_call(
        grads_kernel,
        grid=(width // step,),
        out_shape=[jax.ShapeDtypeStruct((hid, width), BF)] * 3 + small,
        in_specs=[pl.BlockSpec((2, total, step), lambda i: (0, 0, i)), held(kept_dt.shape)]
        + [held(s.shape) for s in small],
        out_specs=[weights] * 3 + [held(s.shape) for s in small],
        name="grads",
    )(kept_rows, kept_dt, *results)
    return (grad_gate.T[None], grad_up.T[None], grad_down[None], grad_out, grad_b, grad_c, grad_v)


def solution(mesh):
    nz = mesh.shape["sp"] // NX
    ntp = mesh.shape["tp"]
    tok, tok_tp = P("sp", None), P("sp", "tp")
    return jax.shard_map(
        functools.partial(local, nz, ntp),
        mesh=mesh,
        in_specs=(
            tok_tp,
            tok_tp,
            tok,
            tok,
            P("sp", None, "tp"),
            P("sp", None, "tp"),
            P("sp", "tp", None),
            P(None, "tp"),
            tok_tp,
            tok_tp,
            tok_tp,
            tok_tp,
            P(None, "tp"),
        ),
        out_specs=(
            P("sp", None, "tp"),
            P("sp", None, "tp"),
            P("sp", "tp", None),
            tok_tp,
            tok_tp,
            tok_tp,
            tok_tp,
        ),
        check_vma=False,
    )
```

```python
import functools

import jax
import jax.numpy as jnp
from jax import lax
from jax.experimental import pallas as pl
from jax.experimental.pallas import tpu as pltpu
from jax.sharding import PartitionSpec as P

MESH = pl.DeviceIdType.MESH
NX = 4
NY = 4
BF = jnp.bfloat16
F32 = jnp.float32


def block_order(nz):
    near = [0, 1, nz - 1]
    return near + sorted(set(range(nz)) - set(near), key=lambda d: (-min(d, nz - d), d))


class Place:
    def __init__(self, nz):
        self.nz = nz
        self.sp = lax.axis_index("sp")
        self.tp = lax.axis_index("tp")
        self.z = lax.div(self.sp, NX)
        self.x = lax.rem(self.sp, NX)
        self.y = lax.div(self.tp, 2)
        self.c = lax.rem(self.tp, 2)

    def over_sp(self, dz, dx):
        z = lax.rem(self.z + dz, self.nz)
        x = lax.rem(self.x + dx, NX)
        return (z * NX + x, self.tp)

    def paired(self, dm, dx):
        z = self.z + dm * (1 - 2 * lax.rem(self.z, 2))
        return (z * NX + lax.rem(self.x + dx, NX), self.tp)

    def over_y(self, dy):
        return (self.sp, lax.rem(self.y + dy + NY, NY) * 2 + self.c)

    def other(self):
        return (self.sp, self.y * 2 + 1 - self.c)

    def origin(self, dy, flip):
        y = lax.rem(self.y + dy + NY, NY)
        c = 1 - self.c if flip else self.c
        return y * 2 + c


def greet(here):
    barrier = pltpu.get_barrier_semaphore()
    peers = [here.over_sp(dz, dx) for dz in range(here.nz) for dx in range(NX) if dz or dx]
    peers += [here.other(), here.over_y(1), here.over_y(-1)]
    for peer in peers:
        pl.semaphore_signal(barrier, inc=1, device_id=peer, device_id_type=MESH)
    return barrier, len(peers)


def send(src, dst, send_sem, recv_sem, peer):
    copy = pltpu.make_async_remote_copy(
        src_ref=src,
        dst_ref=dst,
        send_sem=send_sem,
        recv_sem=recv_sem,
        device_id=peer,
        device_id_type=MESH,
    )
    copy.start()


def await_bytes(ref, sem):
    pltpu.make_async_copy(ref, ref, sem).wait()


class Gather:
    def __init__(self, here, chunk, send_sem, near, far, group=lambda h: 0):
        self.here, self.chunk, self.send_sem = here, chunk, send_sem
        self.near, self.far, self.group = near, far, group

    def _send(self, origin, h, peer, recv_sem):
        ref = self.chunk(origin, h)
        send(ref, ref, self.send_sem, recv_sem, peer)

    def start(self, h):
        here = self.here
        mine = here.origin(0, False)
        self._send(mine, h, here.over_y(1), self.near.at[0, h])
        self._send(mine, h, here.over_y(-1), self.near.at[1, h])
        self._send(mine, h, here.other(), self.far.at[0, self.group(h)])

    def forward(self, h):
        here = self.here
        low, high = here.origin(-1, False), here.origin(1, False)
        await_bytes(self.chunk(low, h), self.near.at[0, h])
        if h % 2 == 0:
            self._send(low, h, here.over_y(1), self.near.at[2, h])
        self._send(low, h, here.other(), self.far.at[1, self.group(h)])
        await_bytes(self.chunk(high, h), self.near.at[1, h])
        if h % 2 == 1:
            self._send(high, h, here.over_y(-1), self.near.at[2, h])
        self._send(high, h, here.other(), self.far.at[2, self.group(h)])

    def last(self, h):
        here = self.here
        across = here.origin(2, False)
        await_bytes(self.chunk(across, h), self.near.at[2, h])
        self._send(across, h, here.other(), self.far.at[3, self.group(h)])

    def finish(self, whole, g=0):
        here = self.here
        for k, dy in enumerate((0, -1, 1, 2)):
            await_bytes(whole(here.origin(dy, True)), self.far.at[k, g])


def slots_of(ids, here, total):
    tokens = ids.shape[0]
    lanes = lax.broadcasted_iota(jnp.int32, (tokens, 128), 1)
    named = [(lanes == ids[:, k : k + 1]).astype(F32) for k in range(2)]
    rows = lax.broadcasted_iota(jnp.int32, (tokens, tokens), 0)
    cols = lax.broadcasted_iota(jnp.int32, (tokens, tokens), 1)
    earlier = (cols < rows).astype(F32).astype(BF)
    before = jnp.dot(earlier, (named[0] + named[1]).astype(BF), preferred_element_type=F32)
    cap = total // (here.nz * NX)
    out = []
    for k in range(2):
        slot = jnp.sum(before * named[k], axis=1, keepdims=True)
        e = ids[:, k : k + 1]
        dz = ((e // NX if NX not in (1, 2, 4) else (e >> (NX.bit_length() - 1))) - here.z) & (here.nz - 1)
        dx = ((e & (NX - 1)) - here.x) & (NX - 1)
        out.append(((dz * NX + dx) * cap).astype(F32) + slot)
    return out


def nt(a, b):
    return lax.dot_general(a, b, (((1,), (1,)), ((), ())), preferred_element_type=F32)


def step_kernel(
    nz,
    og_ref,
    x_ref,
    rw_ref,
    ids_ref,
    conv_ref,
    gb_ref,
    gc_ref,
    vv_ref,
    taps_ref,
    wg_hbm,
    wu_hbm,
    wd_hbm,
    op_hbm,
    go_ref,
    gradb_ref,
    gradc_ref,
    gradv_ref,
    gate_ref,
    up_ref,
    down_ref,
    sbuf,
    buf,
    wcat,
    wd,
    out_proj,
    dcat,
    dt,
    part,
    pr,
    sb,
    ra,
    rb,
    sc,
    rc,
    fin,
    ret,
    pick,
    dh,
    dhall,
    dht,
    xall,
    mixed,
    mx,
    edge,
    halo,
    gpart,
    gr,
    w_sem,
    own_sem,
    a_send,
    a_recv,
    g_send,
    g_near,
    g_far,
    pair_send,
    pair_recv,
    rs_send,
    rs_recv,
    sp_send,
    sp_recv,
    dh_send,
    dh_near,
    dh_far,
    xb_send,
    xb_near,
    xb_far,
    x_send,
    x_recv,
    m_send,
    m_recv,
    e_send,
    e_recv,
    z_send,
    z_recv,
):
    here = Place(nz)
    barrier, peers = greet(here)
    total, chans = sbuf.shape[1:]
    cap = total // (nz * NX)
    tokens = og_ref.shape[0]
    hid, padded = wg_hbm.shape[0], wd.shape[0]
    order = block_order(nz)
    at = {d: p for p, d in enumerate(order)}
    rows = NX * cap
    half = total // 2
    hb = nz // 2

    loads = [
        pltpu.make_async_copy(wg_hbm, wcat.at[0:hid, :], w_sem.at[0]),
        pltpu.make_async_copy(wu_hbm, wcat.at[padded : padded + hid, :], w_sem.at[1]),
        pltpu.make_async_copy(wd_hbm, wd.at[0:hid, :], w_sem.at[2]),
        pltpu.make_async_copy(op_hbm, out_proj, w_sem.at[3]),
    ]
    for load in loads:
        load.start()

    ids = ids_ref[...].astype(F32).T.astype(jnp.int32)
    rw = rw_ref[...].T
    slots = slots_of(ids, here, total)
    srow = lax.broadcasted_iota(jnp.int32, (total, tokens), 0).astype(F32)
    places = []
    for k in range(2):
        wide = jnp.broadcast_to(slots[k], (tokens, tokens)).T
        places.append((srow == wide[0:1, :]).astype(F32))
    both = (places[0] + places[1]).astype(BF)
    sbuf[0] = jnp.dot(both, x_ref[...], preferred_element_type=F32).astype(BF)
    og = og_ref[...].astype(F32)
    dy = None
    for k in range(2):
        weighted = (rw[:, k : k + 1] * og).astype(BF)
        term = jnp.dot(places[k].astype(BF), weighted, preferred_element_type=F32)
        dy = term if dy is None else dy + term
    sbuf[1] = dy.astype(BF)

    def cols(origin):
        return pl.ds(pl.multiple_of(origin * chans, chans), chans)

    column = cols(here.tp)
    pl.semaphore_wait(barrier, peers)
    own = pltpu.make_async_copy(sbuf.at[:, 0:cap, :], buf.at[:, 0:cap, column], own_sem.at[5])
    own.start()
    for dz in order:
        for dx in range(NX):
            if dz or dx:
                r = (dz * NX + dx) * cap
                p = at[(-dz) % nz]
                t = p * rows + ((-dx) % NX) * cap
                send(
                    sbuf.at[:, pl.ds(r, cap), :],
                    buf.at[:, pl.ds(t, cap), column],
                    a_send,
                    a_recv.at[p],
                    here.over_sp(dz, dx),
                )
    scol = lax.broadcasted_iota(jnp.int32, (tokens, total), 1).astype(F32)
    pick[...] = ((scol == slots[0]).astype(F32) + (scol == slots[1]).astype(F32)).astype(BF)
    mixed[...] = (gb_ref[...].astype(F32) * conv_ref[...].astype(F32)).astype(BF)
    wcat[hid:padded, :] = jnp.zeros((padded - hid, wcat.shape[1]), BF)
    wcat[padded + hid :, :] = jnp.zeros((padded - hid, wcat.shape[1]), BF)
    wd[hid:, :] = jnp.zeros((padded - hid, wcat.shape[1]), BF)

    side = lax.rem(here.z, 2)
    family = [(dm, dx) for dm in range(2) for dx in range(NX) if dm or dx]
    seat = pl.ds(pl.multiple_of((side * NX + here.x) * tokens, tokens), tokens)
    own_mixed = pltpu.make_async_copy(mixed, mx.at[seat, :], own_sem.at[0])
    own_mixed.start()

    def chunk(origin, h):
        return buf.at[:, pl.ds(h * rows, rows), cols(origin)]

    gather = Gather(here, chunk, g_send, g_near, g_far, lambda h: h // hb)

    def experts(r0, n):
        r = pl.ds(r0, n)
        gu = nt(buf[0, r, :], wcat[...])
        dhid = nt(buf[1, r, :], wd[...])
        gate, upval = gu[:, :padded], gu[:, padded:]
        sig = jax.nn.sigmoid(gate)
        act = gate * sig
        dcat[r, 0:padded] = (dhid * upval * (sig * (1.0 + gate * (1.0 - sig)))).astype(BF)
        dcat[r, padded : 2 * padded] = (dhid * act).astype(BF)
        dcat[r, 2 * padded :] = (act * upval).astype(BF)

    def whole(k):
        return lambda origin: buf.at[:, pl.ds(k * half, half), cols(origin)]

    def spread(k):
        r = pl.ds(k * half, half)
        d = dcat[r, 0 : 2 * padded]
        step = 2 * chans
        for n in range(NY):
            c = pl.ds(n * step, step)
            part[r, c] = jnp.dot(d, wcat[:, c], preferred_element_type=F32).astype(BF)
        for y in range(NY):
            send(
                part.at[r, cols(2 * y + 1 - here.c)],
                pr.at[y, r, :],
                pair_send,
                pair_recv.at[k],
                here.other(),
            )

    def pair(p, dy):
        y = lax.rem(here.y + dy + NY, NY)
        r = pl.ds(p * rows, rows)
        return part[r, cols(2 * y + here.c)].astype(F32) + pr[y, r, :].astype(F32)

    def stage_a(p):
        way = 1 if p % 2 == 0 else -1
        r = pl.ds(p * rows, rows)
        sb[0, r, :] = pair(p, 2).astype(BF)
        send(sb.at[0, r, :], ra.at[r, :], rs_send.at[0], rs_recv.at[0, p], here.over_y(way))
        sb[1, r, :] = pair(p, -way).astype(BF)
        send(sb.at[1, r, :], rb.at[r, :], rs_send.at[1], rs_recv.at[1, p], here.over_y(-way))

    def stage_b(p):
        way = 1 if p % 2 == 0 else -1
        r = pl.ds(p * rows, rows)
        await_bytes(ra.at[r, :], rs_recv.at[0, p])
        sc[r, :] = (pair(p, way) + ra[r, :].astype(F32)).astype(BF)
        send(sc.at[r, :], rc.at[r, :], rs_send.at[2], rs_recv.at[2, p], here.over_y(way))

    def stage_c(p):
        r = pl.ds(p * rows, rows)
        await_bytes(rb.at[r, :], rs_recv.at[1, p])
        await_bytes(rc.at[r, :], rs_recv.at[2, p])
        fin[r, :] = (pair(p, 0) + rb[r, :].astype(F32) + rc[r, :].astype(F32)).astype(BF)
        dz = order[p]
        for dx in range(NX):
            src = fin.at[pl.ds(p * rows + dx * cap, cap), :]
            t = (((-dz) % nz) * NX + (-dx) % NX) * cap
            dst = ret.at[pl.ds(t, cap), :]
            if dz or dx:
                send(src, dst, sp_send, sp_recv, here.over_sp(dz, dx))

    def pair_arrived(k):
        await_bytes(pr.at[:, pl.ds(k * half, half), :], pair_recv.at[k])

    first = list(range(hb - 1, -1, -1))
    second = list(range(hb, nz))
    for p in range(nz + LAST):
        if p < nz:
            if p == 0:
                own.wait()
                await_bytes(buf.at[:, cap:rows, column], a_recv.at[0])
            else:
                await_bytes(buf.at[:, pl.ds(p * rows, rows), column], a_recv.at[p])
            gather.start(p)
        if p == nz - 1:
            for dm, dx in family:
                send(mixed, mx.at[seat, :], m_send, m_recv, here.paired(dm, dx))
        if 0 <= p - FORWARD < nz:
            gather.forward(p - FORWARD)
        if p == nz - 1 + FORWARD:
            gather.finish(whole(0), 0)
            for load in loads[:3]:
                load.wait()
            experts(0, half)
        if 0 <= p - LAST < nz:
            gather.last(p - LAST)
        if p == nz + FORWARD:
            spread(0)
    pair_arrived(0)
    for p in first:
        stage_a(p)
    gather.finish(whole(1), 1)
    experts(half, half)
    spread(1)
    for p in first:
        stage_b(p)
    pair_arrived(1)
    for p in second:
        stage_a(p)
    slab = 3 * padded // 9

    def turn(k):
        dt[k * slab : (k + 1) * slab, :] = dcat[:, k * slab : (k + 1) * slab].astype(F32).T.astype(BF)

    def weights(n):
        c = pl.ds(n * chans, chans)
        both = jnp.dot(dt[0 : 2 * padded, :], buf[0, :, c], preferred_element_type=F32)
        gate_ref[:, c] = both[0:hid, :].astype(BF)
        up_ref[:, c] = both[padded : padded + hid, :].astype(BF)
        down_ref[:, c] = jnp.dot(dt[2 * padded :, :], buf[1, :, c], preferred_element_type=F32)[0:hid, :].astype(BF)

    for p in first:
        stage_c(p)
    for k in range(9):
        turn(k)
    for p in second:
        stage_b(p)
    for p in second:
        stage_c(p)
    ret[0:cap, :] = fin[0:cap, :]
    for n in range(3):
        weights(n)
    await_bytes(ret.at[pl.ds(cap, total - cap), :], sp_recv)

    moe = jnp.dot(pick[...], ret[...], preferred_element_type=F32)
    grad_h = og_ref[...].astype(F32) + moe
    dht[...] = grad_h.T.astype(BF)
    dh[...] = grad_h.astype(BF)

    wide = chans // NX
    piece = wide // 2
    tcol = pl.ds(pl.multiple_of((side * NX + here.x) * tokens, tokens), tokens)

    def orows(origin, h=0, n=1):
        size = piece // n
        return pl.ds(pl.multiple_of(origin * piece + h * size, size), size)

    def share(m, x):
        return pl.ds(pl.multiple_of(x * wide + m * piece, piece), piece)

    mine = orows(here.tp)
    for dm, dx in family:
        m = lax.rem(side + dm, 2)
        send(
            dht.at[share(m, lax.rem(here.x + dx, NX)), :],
            xall.at[mine, tcol],
            x_send,
            x_recv,
            here.paired(dm, dx),
        )
    own_x = pltpu.make_async_copy(dht.at[share(side, here.x), :], xall.at[mine, tcol], own_sem.at[1])
    own_x.start()
    own_dh = pltpu.make_async_copy(dh, dhall.at[:, column], own_sem.at[2])
    own_dh.start()
    own_dh.wait()
    ht = tokens // 2
    dh_gather = Gather(here, lambda o, h: dhall.at[pl.ds(h * ht, ht), cols(o)], dh_send, dh_near, dh_far)
    xb_gather = Gather(here, lambda o, h: xall.at[orows(o, h, 2), :], xb_send, xb_near, xb_far)
    dh_gather.start(0)
    dh_gather.start(1)
    weights(3)
    own_x.wait()
    await_bytes(xall.at[pl.ds(0, piece), pl.ds(0, len(family) * tokens)], x_recv)
    xb_gather.start(0)
    xb_gather.start(1)
    weights(4)
    weights(5)
    for h in range(2):
        dh_gather.forward(h)
    for h in range(2):
        xb_gather.forward(h)
    for h in range(2):
        dh_gather.last(h)
    for h in range(2):
        xb_gather.last(h)
    own_mixed.wait()
    await_bytes(mx.at[pl.ds(0, len(family) * tokens), :], m_recv)
    xb_gather.finish(lambda o: xall.at[orows(o), :])
    gpart[...] = jnp.dot(xall[...], mx[...], preferred_element_type=F32).astype(BF)
    for dz in order[1:]:
        to = lax.rem(here.z + dz, nz)
        send(gpart.at[orows(to), :], gr.at[dz], z_send, z_recv, here.over_sp(dz, 0))
    own_g = pltpu.make_async_copy(gpart.at[orows(here.z), :], gr.at[0], own_sem.at[4])
    own_g.start()

    dh_gather.finish(lambda o: dhall.at[:, cols(o)])
    loads[3].wait()
    grad_z = jnp.dot(dhall[...], out_proj[...], preferred_element_type=F32)
    dconv = (grad_z * gb_ref[...].astype(F32)).astype(BF)
    edge[0, :, :] = dconv[0:16, :]
    edge[1, :, :] = dconv[tokens - 16 :, :]
    last_sp = nz * NX
    before = (lax.rem(here.sp + last_sp - 1, last_sp), here.tp)
    after = (lax.rem(here.sp + 1, last_sp), here.tp)
    send(edge.at[0], halo.at[1], e_send.at[0], e_recv.at[1], before)
    send(edge.at[1], halo.at[0], e_send.at[1], e_recv.at[0], after)
    gradb_ref[...] = (grad_z * conv_ref[...].astype(F32)).astype(BF)
    for n in range(6, 2 * NY):
        weights(n)
    await_bytes(halo.at[0], e_recv.at[0])
    await_bytes(halo.at[1], e_recv.at[1])
    dconv = dconv.astype(F32)
    row = lax.broadcasted_iota(jnp.int32, dconv.shape, 0)
    low = halo[0].astype(F32)[15:16, :] * (here.sp > 0).astype(F32)
    high = halo[1].astype(F32)[0:1, :] * (here.sp < last_sp - 1).astype(F32)
    prev = jnp.where(row == 0, low, pltpu.roll(dconv, 1, 0))
    nxt = jnp.where(row == tokens - 1, high, pltpu.roll(dconv, tokens - 1, 0))
    grad_u = taps_ref[0:1, :] * nxt + taps_ref[1:2, :] * dconv + taps_ref[2:3, :] * prev
    gradc_ref[...] = (grad_u * vv_ref[...].astype(F32)).astype(BF)
    gradv_ref[...] = (grad_u * gc_ref[...].astype(F32)).astype(BF)

    others = 2 * NY - 1
    await_bytes(sbuf.at[:, pl.ds(0, total - cap), :], a_send)
    await_bytes(buf.at[:, pl.ds(0, total - total // (2 * NY)), :], g_send)
    await_bytes(pr, pair_send)
    for k in range(3):
        await_bytes(ra, rs_send.at[k])
    await_bytes(ret.at[pl.ds(cap, total - cap), :], sp_send)
    await_bytes(dhall.at[:, pl.ds(0, others * chans)], dh_send)
    await_bytes(xall.at[pl.ds(0, others * piece), :], xb_send)
    await_bytes(xall.at[pl.ds(0, piece), pl.ds(0, len(family) * tokens)], x_send)
    await_bytes(mx.at[pl.ds(0, len(family) * tokens), :], m_send)
    await_bytes(edge.at[0], e_send.at[0])
    await_bytes(edge.at[1], e_send.at[1])

    own_g.wait()
    await_bytes(gr.at[pl.ds(1, nz - 1)], z_recv)
    for m in range(2):
        summed = gr[m].astype(F32)
        for k in range(m + 2, nz, 2):
            summed = summed + gr[k].astype(F32)
        go_ref[pl.ds(pl.multiple_of(lax.rem(side + m, 2) * piece, piece), piece), :] = summed
    await_bytes(gr.at[pl.ds(1, nz - 1)], z_send)


def write_kernel(*refs):
    count = len(refs) // 2
    sems = refs[-1]
    copies = [pltpu.make_async_copy(refs[k], refs[count + k], sems.at[k]) for k in range(count)]
    for copy in copies:
        copy.start()
    for copy in copies:
        copy.wait()


VM = pl.BlockSpec(memory_space=pltpu.VMEM)
ANY = pl.BlockSpec(memory_space=pl.ANY)
FORWARD, LAST = 2, 4


def local(
    nz,
    ntp,
    out_grad,
    moe_input,
    route_weight,
    route_ids,
    gate_proj,
    up_proj,
    down_proj,
    out_proj,
    conv_out,
    gate_b,
    gate_c,
    value_v,
    conv_taps,
):
    tokens, chans = out_grad.shape
    ns = nz * NX
    cap = 4 * tokens // ns
    total = ns * cap
    width = chans * ntp
    hid = gate_proj.shape[2]
    padded = -(-hid // 128) * 128
    wide = chans // NX
    dma = pltpu.SemaphoreType.DMA

    def vm(*shape):
        return pltpu.VMEM(shape, BF)

    small = [
        jax.ShapeDtypeStruct((wide, chans), F32),
        jax.ShapeDtypeStruct((tokens, chans), BF),
        jax.ShapeDtypeStruct((tokens, chans), BF),
        jax.ShapeDtypeStruct((tokens, chans), BF),
    ]
    held = [(a.shape, a.dtype) for a in small]
    held += [((hid, width), BF)] * 3
    results = pl.pallas_call(
        functools.partial(step_kernel, nz),
        out_shape=[pltpu.VMEM(*h) for h in held],
        in_specs=[VM] * 9 + [ANY] * 4,
        out_specs=[VM] * 7,
        scratch_shapes=[
            vm(2, total, chans),
            vm(2, total, width),
            vm(2 * padded, width),
            vm(padded, width),
            vm(width, chans),
            vm(total, 3 * padded),
            vm(3 * padded, total),
            vm(total, width),
            vm(NY, total, chans),
            vm(2, total, chans),
            vm(total, chans),
            vm(total, chans),
            vm(total, chans),
            vm(total, chans),
            vm(total, chans),
            vm(total, chans),
            vm(tokens, total),
            vm(tokens, chans),
            vm(tokens, width),
            vm(chans, tokens),
            vm(ntp * wide // 2, 2 * NX * tokens),
            vm(tokens, chans),
            vm(2 * NX * tokens, chans),
            vm(2, 16, chans),
            vm(2, 16, chans),
            vm(nz * wide // 2, chans),
            vm(nz, wide // 2, chans),
            dma((4,)),
            dma((7,)),
            dma,
            dma((nz,)),
            dma,
            dma((3, nz)),
            dma((4, 2)),
            dma,
            dma((2,)),
            dma((3,)),
            dma((3, nz)),
            dma,
            dma,
            dma,
            dma((3, 2)),
            dma((4, 1)),
            dma,
            dma((3, 2)),
            dma((4, 1)),
            dma,
            dma,
            dma,
            dma,
            dma((2,)),
            dma((2,)),
            dma,
            dma,
        ],
        compiler_params=pltpu.CompilerParams(
            collective_id=0, has_side_effects=True, vmem_limit_bytes=40 * 1024 * 1024
        ),
        name="step",
    )(
        *(
            pltpu.with_memory_space_constraint(a, pltpu.HBM)
            for a in (
                out_grad,
                moe_input,
                route_weight.T,
                route_ids.T,
                conv_out,
                gate_b,
                gate_c,
                value_v,
                conv_taps,
                gate_proj[0].T,
                up_proj[0].T,
                down_proj[0],
                out_proj,
            )
        )
    )
    grad_out, grad_b, grad_c, grad_v, grad_gate, grad_up, grad_down = pl.pallas_call(
        write_kernel,
        out_shape=[jax.ShapeDtypeStruct(*h) for h in held],
        in_specs=[VM] * 7,
        out_specs=[ANY] * 7,
        scratch_shapes=[dma((7,))],
        compiler_params=pltpu.CompilerParams(vmem_limit_bytes=8 * 1024 * 1024),
        name="write",
    )(*[pltpu.with_memory_space_constraint(r, pltpu.VMEM) for r in results])
    return (grad_gate.T[None], grad_up.T[None], grad_down[None], grad_out, grad_b, grad_c, grad_v)


def solution(mesh):
    nz = mesh.shape["sp"] // NX
    ntp = mesh.shape["tp"]
    tok, tok_tp = P("sp", None), P("sp", "tp")
    return jax.shard_map(
        functools.partial(local, nz, ntp),
        mesh=mesh,
        in_specs=(
            tok_tp,
            tok_tp,
            tok,
            tok,
            P("sp", None, "tp"),
            P("sp", None, "tp"),
            P("sp", "tp", None),
            P(None, "tp"),
            tok_tp,
            tok_tp,
            tok_tp,
            tok_tp,
            P(None, "tp"),
        ),
        out_specs=(
            P("sp", None, "tp"),
            P("sp", None, "tp"),
            P("sp", "tp", None),
            tok_tp,
            tok_tp,
            tok_tp,
            tok_tp,
        ),
        check_vma=False,
    )
```

```python
import functools

import jax
import jax.numpy as jnp
from jax import lax
from jax.experimental import pallas as pl
from jax.experimental.pallas import tpu as pltpu
from jax.sharding import PartitionSpec as P

MESH = pl.DeviceIdType.MESH
NX = 4
NY = 4
BF = jnp.bfloat16
F32 = jnp.float32


def block_order(nz):
    near = [0, 1, nz - 1]
    return near + sorted(set(range(nz)) - set(near), key=lambda d: (-min(d, nz - d), d))


class Place:
    def __init__(self, nz):
        self.nz = nz
        self.sp = lax.axis_index("sp")
        self.tp = lax.axis_index("tp")
        self.z = lax.div(self.sp, NX)
        self.x = lax.rem(self.sp, NX)
        self.y = lax.div(self.tp, 2)
        self.c = lax.rem(self.tp, 2)

    def over_sp(self, dz, dx):
        z = lax.rem(self.z + dz, self.nz)
        x = lax.rem(self.x + dx, NX)
        return (z * NX + x, self.tp)

    def paired(self, dm, dx):
        z = self.z + dm * (1 - 2 * lax.rem(self.z, 2))
        return (z * NX + lax.rem(self.x + dx, NX), self.tp)

    def over_y(self, dy):
        return (self.sp, lax.rem(self.y + dy + NY, NY) * 2 + self.c)

    def other(self):
        return (self.sp, self.y * 2 + 1 - self.c)

    def origin(self, dy, flip):
        y = lax.rem(self.y + dy + NY, NY)
        c = 1 - self.c if flip else self.c
        return y * 2 + c


def greet(here):
    barrier = pltpu.get_barrier_semaphore()
    peers = [here.over_sp(dz, dx) for dz in range(here.nz) for dx in range(NX) if dz or dx]
    peers += [here.other(), here.over_y(1), here.over_y(-1), here.over_y(2)]
    for peer in peers:
        pl.semaphore_signal(barrier, inc=1, device_id=peer, device_id_type=MESH)
    return barrier, len(peers)


def send(src, dst, send_sem, recv_sem, peer):
    copy = pltpu.make_async_remote_copy(
        src_ref=src,
        dst_ref=dst,
        send_sem=send_sem,
        recv_sem=recv_sem,
        device_id=peer,
        device_id_type=MESH,
    )
    copy.start()


def await_bytes(ref, sem):
    pltpu.make_async_copy(ref, ref, sem).wait()


class Gather:
    def __init__(self, here, chunk, send_sem, near, far, group=lambda h: 0, direct=False):
        self.here, self.chunk, self.send_sem = here, chunk, send_sem
        self.near, self.far, self.group, self.direct = near, far, group, direct

    def _send(self, origin, h, peer, recv_sem):
        ref = self.chunk(origin, h)
        send(ref, ref, self.send_sem, recv_sem, peer)

    def start(self, h):
        here = self.here
        mine = here.origin(0, False)
        self._send(mine, h, here.over_y(1), self.near.at[0, h])
        self._send(mine, h, here.over_y(-1), self.near.at[1, h])
        if self.direct:
            self._send(mine, h, here.over_y(2), self.near.at[2, h])
        self._send(mine, h, here.other(), self.far.at[0, self.group(h)])

    def forward(self, h):
        here = self.here
        low, high = here.origin(-1, False), here.origin(1, False)
        await_bytes(self.chunk(low, h), self.near.at[0, h])
        if h % 2 == 0 and not self.direct:
            self._send(low, h, here.over_y(1), self.near.at[2, h])
        self._send(low, h, here.other(), self.far.at[1, self.group(h)])
        await_bytes(self.chunk(high, h), self.near.at[1, h])
        if h % 2 == 1 and not self.direct:
            self._send(high, h, here.over_y(-1), self.near.at[2, h])
        self._send(high, h, here.other(), self.far.at[2, self.group(h)])

    def last(self, h):
        here = self.here
        across = here.origin(2, False)
        await_bytes(self.chunk(across, h), self.near.at[2, h])
        self._send(across, h, here.other(), self.far.at[3, self.group(h)])

    def finish(self, whole, g=0):
        here = self.here
        for k, dy in enumerate((0, -1, 1, 2)):
            await_bytes(whole(here.origin(dy, True)), self.far.at[k, g])


def slots_of(ids, here, total):
    tokens = ids.shape[0]
    lanes = lax.broadcasted_iota(jnp.int32, (tokens, 128), 1)
    named = [(lanes == ids[:, k : k + 1]).astype(F32) for k in range(2)]
    rows = lax.broadcasted_iota(jnp.int32, (tokens, tokens), 0)
    cols = lax.broadcasted_iota(jnp.int32, (tokens, tokens), 1)
    earlier = (cols < rows).astype(F32).astype(BF)
    before = jnp.dot(earlier, (named[0] + named[1]).astype(BF), preferred_element_type=F32)
    cap = total // (here.nz * NX)
    out = []
    for k in range(2):
        slot = jnp.sum(before * named[k], axis=1, keepdims=True)
        e = ids[:, k : k + 1]
        dz = ((e // NX if NX not in (1, 2, 4) else (e >> (NX.bit_length() - 1))) - here.z) & (here.nz - 1)
        dx = ((e & (NX - 1)) - here.x) & (NX - 1)
        out.append(((dz * NX + dx) * cap).astype(F32) + slot)
    return out


def nt(a, b):
    return lax.dot_general(a, b, (((1,), (1,)), ((), ())), preferred_element_type=F32)


def step_kernel(
    nz,
    og_hbm,
    x_hbm,
    rw_hbm,
    ids_hbm,
    conv_hbm,
    gb_hbm,
    gc_hbm,
    vv_hbm,
    taps_hbm,
    wg_hbm,
    wu_hbm,
    wd_hbm,
    op_hbm,
    go_ref,
    gradb_ref,
    gradc_ref,
    gradv_ref,
    gate_ref,
    up_ref,
    down_ref,
    og_ref,
    x_ref,
    rw_ref,
    ids_ref,
    conv_ref,
    gb_ref,
    gc_ref,
    vv_ref,
    taps_ref,
    sbuf,
    buf,
    wcat,
    wd,
    out_proj,
    dcat,
    dt,
    part,
    pr,
    sb,
    ra,
    rb,
    sc,
    rc,
    fin,
    ret,
    pick,
    dh,
    dhall,
    dht,
    xall,
    mixed,
    mx,
    edge,
    halo,
    gpart,
    gr,
    i_sem,
    w_sem,
    own_sem,
    a_send,
    a_recv,
    g_send,
    g_near,
    g_far,
    pair_send,
    pair_recv,
    rs_send,
    rs_recv,
    sp_send,
    sp_recv,
    dh_send,
    dh_near,
    dh_far,
    xb_send,
    xb_near,
    xb_far,
    x_send,
    x_recv,
    m_send,
    m_recv,
    e_send,
    e_recv,
    z_send,
    z_recv,
):
    here = Place(nz)
    barrier, peers = greet(here)
    total, chans = sbuf.shape[1:]
    cap = total // (nz * NX)
    tokens = og_ref.shape[0]
    hid, padded = wg_hbm.shape[0], wd.shape[0]
    order = block_order(nz)
    at = {d: p for p, d in enumerate(order)}
    rows = NX * cap
    half = total // 2
    hb = nz // 2

    inputs = [
        pltpu.make_async_copy(a, b, i_sem.at[k])
        for k, (a, b) in enumerate(
            [
                (ids_hbm, ids_ref),
                (rw_hbm, rw_ref),
                (x_hbm, x_ref),
                (og_hbm, og_ref),
                (gb_hbm, gb_ref),
                (conv_hbm, conv_ref),
                (gc_hbm, gc_ref),
                (vv_hbm, vv_ref),
                (taps_hbm, taps_ref),
            ]
        )
    ]
    for load in inputs:
        load.start()
    loads = [
        pltpu.make_async_copy(wg_hbm, wcat.at[0:hid, :], w_sem.at[0]),
        pltpu.make_async_copy(wu_hbm, wcat.at[padded : padded + hid, :], w_sem.at[1]),
        pltpu.make_async_copy(wd_hbm, wd.at[0:hid, :], w_sem.at[2]),
        pltpu.make_async_copy(op_hbm, out_proj, w_sem.at[3]),
    ]
    for load in loads:
        load.start()

    inputs[0].wait()
    ids = ids_ref[...].astype(F32).T.astype(jnp.int32)
    slots = slots_of(ids, here, total)
    srow = lax.broadcasted_iota(jnp.int32, (total, tokens), 0).astype(F32)
    places = []
    for k in range(2):
        wide = jnp.broadcast_to(slots[k], (tokens, tokens)).T
        places.append((srow == wide[0:1, :]).astype(F32))
    both = (places[0] + places[1]).astype(BF)
    for load in inputs[1:4]:
        load.wait()
    rw = rw_ref[...].T
    sbuf[0] = jnp.dot(both, x_ref[...], preferred_element_type=F32).astype(BF)
    og = og_ref[...].astype(F32)
    dy = None
    for k in range(2):
        weighted = (rw[:, k : k + 1] * og).astype(BF)
        term = jnp.dot(places[k].astype(BF), weighted, preferred_element_type=F32)
        dy = term if dy is None else dy + term
    sbuf[1] = dy.astype(BF)

    def cols(origin):
        return pl.ds(pl.multiple_of(origin * chans, chans), chans)

    column = cols(here.tp)
    pl.semaphore_wait(barrier, peers)
    own = pltpu.make_async_copy(sbuf.at[:, 0:cap, :], buf.at[:, 0:cap, column], own_sem.at[5])
    own.start()
    for dz in order:
        for dx in range(NX):
            if dz or dx:
                r = (dz * NX + dx) * cap
                p = at[(-dz) % nz]
                t = p * rows + ((-dx) % NX) * cap
                send(
                    sbuf.at[:, pl.ds(r, cap), :],
                    buf.at[:, pl.ds(t, cap), column],
                    a_send,
                    a_recv.at[p],
                    here.over_sp(dz, dx),
                )
    scol = lax.broadcasted_iota(jnp.int32, (tokens, total), 1).astype(F32)
    pick[...] = ((scol == slots[0]).astype(F32) + (scol == slots[1]).astype(F32)).astype(BF)
    for load in inputs[4:]:
        load.wait()
    mixed[...] = (gb_ref[...].astype(F32) * conv_ref[...].astype(F32)).astype(BF)
    wcat[hid:padded, :] = jnp.zeros((padded - hid, wcat.shape[1]), BF)
    wcat[padded + hid :, :] = jnp.zeros((padded - hid, wcat.shape[1]), BF)
    wd[hid:, :] = jnp.zeros((padded - hid, wcat.shape[1]), BF)

    side = lax.rem(here.z, 2)
    family = [(dm, dx) for dm in range(2) for dx in range(NX) if dm or dx]
    seat = pl.ds(pl.multiple_of((side * NX + here.x) * tokens, tokens), tokens)
    own_mixed = pltpu.make_async_copy(mixed, mx.at[seat, :], own_sem.at[0])
    own_mixed.start()

    def chunk(origin, h):
        return buf.at[:, pl.ds(h * rows, rows), cols(origin)]

    gather = Gather(here, chunk, g_send, g_near, g_far, lambda h: h // hb)

    def experts(r0, n):
        r = pl.ds(r0, n)
        gu = nt(buf[0, r, :], wcat[...])
        dhid = nt(buf[1, r, :], wd[...])
        gate, upval = gu[:, :padded], gu[:, padded:]
        sig = jax.nn.sigmoid(gate)
        act = gate * sig
        dcat[r, 0:padded] = (dhid * upval * (sig * (1.0 + gate * (1.0 - sig)))).astype(BF)
        dcat[r, padded : 2 * padded] = (dhid * act).astype(BF)
        dcat[r, 2 * padded :] = (act * upval).astype(BF)

    def whole(k):
        return lambda origin: buf.at[:, pl.ds(k * half, half), cols(origin)]

    def spread(k):
        r = pl.ds(k * half, half)
        d = dcat[r, 0 : 2 * padded]
        for first_y in range(0, NY, 2):
            for y in range(first_y, first_y + 2):
                c = pl.ds(2 * y * chans, 2 * chans)
                part[r, c] = jnp.dot(d, wcat[:, c], preferred_element_type=F32).astype(BF)
            for y in range(first_y, first_y + 2):
                at = cols(2 * y + 1 - here.c)
                send(part.at[r, at], pr.at[y, r, :], pair_send, pair_recv.at[k], here.other())

    def pair(p, dy):
        y = lax.rem(here.y + dy + NY, NY)
        r = pl.ds(p * rows, rows)
        return part[r, cols(2 * y + here.c)].astype(F32) + pr[y, r, :].astype(F32)

    def stage_a(p):
        way = 1 if p % 2 == 0 else -1
        r = pl.ds(p * rows, rows)
        sb[0, r, :] = pair(p, 2).astype(BF)
        send(sb.at[0, r, :], ra.at[r, :], rs_send.at[0], rs_recv.at[0, p], here.over_y(way))
        sb[1, r, :] = pair(p, -way).astype(BF)
        send(sb.at[1, r, :], rb.at[r, :], rs_send.at[1], rs_recv.at[1, p], here.over_y(-way))

    def stage_b(p):
        way = 1 if p % 2 == 0 else -1
        r = pl.ds(p * rows, rows)
        await_bytes(ra.at[r, :], rs_recv.at[0, p])
        sc[r, :] = (pair(p, way) + ra[r, :].astype(F32)).astype(BF)
        send(sc.at[r, :], rc.at[r, :], rs_send.at[2], rs_recv.at[2, p], here.over_y(way))

    def stage_c(p):
        r = pl.ds(p * rows, rows)
        await_bytes(rb.at[r, :], rs_recv.at[1, p])
        await_bytes(rc.at[r, :], rs_recv.at[2, p])
        fin[r, :] = (pair(p, 0) + rb[r, :].astype(F32) + rc[r, :].astype(F32)).astype(BF)
        dz = order[p]
        for dx in range(NX):
            src = fin.at[pl.ds(p * rows + dx * cap, cap), :]
            t = (((-dz) % nz) * NX + (-dx) % NX) * cap
            dst = ret.at[pl.ds(t, cap), :]
            if dz or dx:
                send(src, dst, sp_send, sp_recv, here.over_sp(dz, dx))

    def pair_arrived(k):
        await_bytes(pr.at[:, pl.ds(k * half, half), :], pair_recv.at[k])

    first = list(range(hb - 1, -1, -1))
    second = list(range(hb, nz))
    for p in range(nz + LAST):
        if p < nz:
            if p == 0:
                own.wait()
                await_bytes(buf.at[:, cap:rows, column], a_recv.at[0])
            else:
                await_bytes(buf.at[:, pl.ds(p * rows, rows), column], a_recv.at[p])
            gather.start(p)
        if p == nz - 1:
            for dm, dx in family:
                send(mixed, mx.at[seat, :], m_send, m_recv, here.paired(dm, dx))
        if 0 <= p - FORWARD < nz:
            gather.forward(p - FORWARD)
        if p == EXPERTS_AT:
            gather.finish(whole(0), 0)
            for load in loads[:3]:
                load.wait()
            experts(0, half)
        if 0 <= p - LAST < nz:
            gather.last(p - LAST)
        if p == SPREAD_AT:
            spread(0)
    pair_arrived(0)
    for p in first:
        stage_a(p)
    gather.finish(whole(1), 1)
    experts(half, half)
    spread(1)
    for p in first:
        stage_b(p)
    pair_arrived(1)
    for p in second:
        stage_a(p)
    slab = 3 * padded // 9

    def turn(k):
        dt[k * slab : (k + 1) * slab, :] = dcat[:, k * slab : (k + 1) * slab].astype(F32).T.astype(BF)

    def weights(n):
        c = pl.ds(n * chans, chans)
        both = jnp.dot(dt[0 : 2 * padded, :], buf[0, :, c], preferred_element_type=F32)
        gate_ref[:, c] = both[0:hid, :].astype(BF)
        up_ref[:, c] = both[padded : padded + hid, :].astype(BF)
        down_ref[:, c] = jnp.dot(dt[2 * padded :, :], buf[1, :, c], preferred_element_type=F32)[0:hid, :].astype(BF)

    for p in first:
        stage_c(p)
    for k in range(9):
        turn(k)
    for p in second:
        stage_b(p)
    for p in second:
        stage_c(p)
    ret[0:cap, :] = fin[0:cap, :]
    for n in range(3):
        weights(n)
    await_bytes(ret.at[pl.ds(cap, total - cap), :], sp_recv)

    moe = jnp.dot(pick[...], ret[...], preferred_element_type=F32)
    grad_h = og_ref[...].astype(F32) + moe
    dht[...] = grad_h.T.astype(BF)
    dh[...] = grad_h.astype(BF)

    wide = chans // NX
    piece = wide // 2
    tcol = pl.ds(pl.multiple_of((side * NX + here.x) * tokens, tokens), tokens)

    def orows(origin, h=0, n=1):
        size = piece // n
        return pl.ds(pl.multiple_of(origin * piece + h * size, size), size)

    def share(m, x):
        return pl.ds(pl.multiple_of(x * wide + m * piece, piece), piece)

    mine = orows(here.tp)
    for dm, dx in family:
        m = lax.rem(side + dm, 2)
        send(
            dht.at[share(m, lax.rem(here.x + dx, NX)), :],
            xall.at[mine, tcol],
            x_send,
            x_recv,
            here.paired(dm, dx),
        )
    own_x = pltpu.make_async_copy(dht.at[share(side, here.x), :], xall.at[mine, tcol], own_sem.at[1])
    own_x.start()
    own_dh = pltpu.make_async_copy(dh, dhall.at[:, column], own_sem.at[2])
    own_dh.start()
    own_dh.wait()
    ht = tokens // 2
    dh_gather = Gather(here, lambda o, h: dhall.at[pl.ds(h * ht, ht), cols(o)], dh_send, dh_near, dh_far)
    xb_gather = Gather(here, lambda o, h: xall.at[orows(o, h, 2), :], xb_send, xb_near, xb_far, direct=DIRECT)
    dh_gather.start(0)
    dh_gather.start(1)
    weights(3)
    own_x.wait()
    await_bytes(xall.at[pl.ds(0, piece), pl.ds(0, len(family) * tokens)], x_recv)
    xb_gather.start(0)
    xb_gather.start(1)
    weights(4)
    weights(5)
    for h in range(2):
        dh_gather.forward(h)
    for h in range(2):
        xb_gather.forward(h)
    for h in range(2):
        dh_gather.last(h)
    for h in range(2):
        xb_gather.last(h)
    dh_gather.finish(lambda o: dhall.at[:, cols(o)])
    loads[3].wait()
    grad_z = jnp.dot(dhall[...], out_proj[...], preferred_element_type=F32)
    dconv = (grad_z * gb_ref[...].astype(F32)).astype(BF)
    edge[0, :, :] = dconv[0:16, :]
    edge[1, :, :] = dconv[tokens - 16 :, :]
    last_sp = nz * NX
    before = (lax.rem(here.sp + last_sp - 1, last_sp), here.tp)
    after = (lax.rem(here.sp + 1, last_sp), here.tp)
    send(edge.at[0], halo.at[1], e_send.at[0], e_recv.at[1], before)
    send(edge.at[1], halo.at[0], e_send.at[1], e_recv.at[0], after)
    gradb_ref[...] = (grad_z * conv_ref[...].astype(F32)).astype(BF)
    own_mixed.wait()
    await_bytes(mx.at[pl.ds(0, len(family) * tokens), :], m_recv)
    xb_gather.finish(lambda o: xall.at[orows(o), :])
    gpart[...] = jnp.dot(xall[...], mx[...], preferred_element_type=F32).astype(BF)
    for dz in sorted(range(1, nz), key=lambda d: -min(d, nz - d)):
        to = lax.rem(here.z + dz, nz)
        send(gpart.at[orows(to), :], gr.at[dz], z_send, z_recv, here.over_sp(dz, 0))
    own_g = pltpu.make_async_copy(gpart.at[orows(here.z), :], gr.at[0], own_sem.at[4])
    own_g.start()

    for n in range(6, 2 * NY):
        weights(n)
    await_bytes(halo.at[0], e_recv.at[0])
    await_bytes(halo.at[1], e_recv.at[1])
    dconv = dconv.astype(F32)
    row = lax.broadcasted_iota(jnp.int32, dconv.shape, 0)
    low = halo[0].astype(F32)[15:16, :] * (here.sp > 0).astype(F32)
    high = halo[1].astype(F32)[0:1, :] * (here.sp < last_sp - 1).astype(F32)
    prev = jnp.where(row == 0, low, pltpu.roll(dconv, 1, 0))
    nxt = jnp.where(row == tokens - 1, high, pltpu.roll(dconv, tokens - 1, 0))
    grad_u = taps_ref[0:1, :] * nxt + taps_ref[1:2, :] * dconv + taps_ref[2:3, :] * prev
    gradc_ref[...] = (grad_u * vv_ref[...].astype(F32)).astype(BF)
    gradv_ref[...] = (grad_u * gc_ref[...].astype(F32)).astype(BF)

    others = 2 * NY - 1
    await_bytes(sbuf.at[:, pl.ds(0, total - cap), :], a_send)
    await_bytes(buf.at[:, pl.ds(0, total - total // (2 * NY)), :], g_send)
    await_bytes(pr, pair_send)
    for k in range(3):
        await_bytes(ra, rs_send.at[k])
    await_bytes(ret.at[pl.ds(cap, total - cap), :], sp_send)
    await_bytes(dhall.at[:, pl.ds(0, others * chans)], dh_send)
    await_bytes(xall.at[pl.ds(0, others * piece), :], xb_send)
    await_bytes(xall.at[pl.ds(0, piece), pl.ds(0, len(family) * tokens)], x_send)
    await_bytes(mx.at[pl.ds(0, len(family) * tokens), :], m_send)
    await_bytes(edge.at[0], e_send.at[0])
    await_bytes(edge.at[1], e_send.at[1])

    own_g.wait()
    await_bytes(gr.at[pl.ds(1, nz - 1)], z_recv)
    for m in range(2):
        summed = gr[m].astype(F32)
        for k in range(m + 2, nz, 2):
            summed = summed + gr[k].astype(F32)
        go_ref[pl.ds(pl.multiple_of(lax.rem(side + m, 2) * piece, piece), piece), :] = summed
    await_bytes(gr.at[pl.ds(1, nz - 1)], z_send)


def write_kernel(*refs):
    count = len(refs) // 2
    sems = refs[-1]
    copies = [pltpu.make_async_copy(refs[k], refs[count + k], sems.at[k]) for k in range(count)]
    for copy in copies:
        copy.start()
    for copy in copies:
        copy.wait()


VM = pl.BlockSpec(memory_space=pltpu.VMEM)
ANY = pl.BlockSpec(memory_space=pl.ANY)
DIRECT = True
FORWARD, LAST = 2, 4
EXPERTS_AT, SPREAD_AT = 8, 9


def local(
    nz,
    ntp,
    out_grad,
    moe_input,
    route_weight,
    route_ids,
    gate_proj,
    up_proj,
    down_proj,
    out_proj,
    conv_out,
    gate_b,
    gate_c,
    value_v,
    conv_taps,
):
    tokens, chans = out_grad.shape
    ns = nz * NX
    cap = 4 * tokens // ns
    total = ns * cap
    width = chans * ntp
    hid = gate_proj.shape[2]
    padded = -(-hid // 128) * 128
    wide = chans // NX
    dma = pltpu.SemaphoreType.DMA

    def vm(*shape):
        return pltpu.VMEM(shape, BF)

    small = [
        jax.ShapeDtypeStruct((wide, chans), F32),
        jax.ShapeDtypeStruct((tokens, chans), BF),
        jax.ShapeDtypeStruct((tokens, chans), BF),
        jax.ShapeDtypeStruct((tokens, chans), BF),
    ]
    held = [(a.shape, a.dtype) for a in small]
    held += [((hid, width), BF)] * 3
    results = pl.pallas_call(
        functools.partial(step_kernel, nz),
        out_shape=[pltpu.VMEM(*h) for h in held],
        in_specs=[ANY] * 13,
        out_specs=[VM] * 7,
        scratch_shapes=[
            vm(tokens, chans),
            vm(tokens, chans),
            pltpu.VMEM((2, tokens), F32),
            pltpu.VMEM((2, tokens), jnp.int32),
            vm(tokens, chans),
            vm(tokens, chans),
            vm(tokens, chans),
            vm(tokens, chans),
            pltpu.VMEM(conv_taps.shape, F32),
            vm(2, total, chans),
            vm(2, total, width),
            vm(2 * padded, width),
            vm(padded, width),
            vm(width, chans),
            vm(total, 3 * padded),
            vm(3 * padded, total),
            vm(total, width),
            vm(NY, total, chans),
            vm(2, total, chans),
            vm(total, chans),
            vm(total, chans),
            vm(total, chans),
            vm(total, chans),
            vm(total, chans),
            vm(total, chans),
            vm(tokens, total),
            vm(tokens, chans),
            vm(tokens, width),
            vm(chans, tokens),
            vm(ntp * wide // 2, 2 * NX * tokens),
            vm(tokens, chans),
            vm(2 * NX * tokens, chans),
            vm(2, 16, chans),
            vm(2, 16, chans),
            vm(nz * wide // 2, chans),
            vm(nz, wide // 2, chans),
            dma((9,)),
            dma((4,)),
            dma((7,)),
            dma,
            dma((nz,)),
            dma,
            dma((3, nz)),
            dma((4, 2)),
            dma,
            dma((2,)),
            dma((3,)),
            dma((3, nz)),
            dma,
            dma,
            dma,
            dma((3, 2)),
            dma((4, 1)),
            dma,
            dma((3, 2)),
            dma((4, 1)),
            dma,
            dma,
            dma,
            dma,
            dma((2,)),
            dma((2,)),
            dma,
            dma,
        ],
        compiler_params=pltpu.CompilerParams(
            collective_id=0, has_side_effects=True, vmem_limit_bytes=40 * 1024 * 1024
        ),
        name="step",
    )(
        *(
            pltpu.with_memory_space_constraint(a, pltpu.HBM)
            for a in (
                out_grad,
                moe_input,
                route_weight.T,
                route_ids.T,
                conv_out,
                gate_b,
                gate_c,
                value_v,
                conv_taps,
                gate_proj[0].T,
                up_proj[0].T,
                down_proj[0],
                out_proj,
            )
        )
    )
    grad_out, grad_b, grad_c, grad_v, grad_gate, grad_up, grad_down = pl.pallas_call(
        write_kernel,
        out_shape=[jax.ShapeDtypeStruct(*h) for h in held],
        in_specs=[VM] * 7,
        out_specs=[ANY] * 7,
        scratch_shapes=[dma((7,))],
        compiler_params=pltpu.CompilerParams(vmem_limit_bytes=8 * 1024 * 1024),
        name="write",
    )(*[pltpu.with_memory_space_constraint(r, pltpu.VMEM) for r in results])
    return (grad_gate.T[None], grad_up.T[None], grad_down[None], grad_out, grad_b, grad_c, grad_v)


def solution(mesh):
    nz = mesh.shape["sp"] // NX
    ntp = mesh.shape["tp"]
    tok, tok_tp = P("sp", None), P("sp", "tp")
    return jax.shard_map(
        functools.partial(local, nz, ntp),
        mesh=mesh,
        in_specs=(
            tok_tp,
            tok_tp,
            tok,
            tok,
            P("sp", None, "tp"),
            P("sp", None, "tp"),
            P("sp", "tp", None),
            P(None, "tp"),
            tok_tp,
            tok_tp,
            tok_tp,
            tok_tp,
            P(None, "tp"),
        ),
        out_specs=(
            P("sp", None, "tp"),
            P("sp", None, "tp"),
            P("sp", "tp", None),
            tok_tp,
            tok_tp,
            tok_tp,
            tok_tp,
        ),
        check_vma=False,
    )
```

```python
import functools

import jax
import jax.numpy as jnp
from jax import lax
from jax.experimental import pallas as pl
from jax.experimental.pallas import tpu as pltpu
from jax.sharding import PartitionSpec as P

MESH = pl.DeviceIdType.MESH
NX = 4
NY = 4
BF = jnp.bfloat16
F32 = jnp.float32


def block_order(nz):
    near = [0, 1, nz - 1]
    return near + sorted(set(range(nz)) - set(near), key=lambda d: (-min(d, nz - d), d))


class Place:
    def __init__(self, nz):
        self.nz = nz
        self.sp = lax.axis_index("sp")
        self.tp = lax.axis_index("tp")
        self.z = lax.div(self.sp, NX)
        self.x = lax.rem(self.sp, NX)
        self.y = lax.div(self.tp, 2)
        self.c = lax.rem(self.tp, 2)

    def over_sp(self, dz, dx):
        z = lax.rem(self.z + dz, self.nz)
        x = lax.rem(self.x + dx, NX)
        return (z * NX + x, self.tp)

    def paired(self, dm, dx):
        z = self.z + dm * (1 - 2 * lax.rem(self.z, 2))
        return (z * NX + lax.rem(self.x + dx, NX), self.tp)

    def over_y(self, dy):
        return (self.sp, lax.rem(self.y + dy + NY, NY) * 2 + self.c)

    def other(self):
        return (self.sp, self.y * 2 + 1 - self.c)

    def origin(self, dy, flip):
        y = lax.rem(self.y + dy + NY, NY)
        c = 1 - self.c if flip else self.c
        return y * 2 + c


def greet(here):
    barrier = pltpu.get_barrier_semaphore()
    peers = [here.over_sp(dz, dx) for dz in range(here.nz) for dx in range(NX) if dz or dx]
    peers += [here.other(), here.over_y(1), here.over_y(-1), here.over_y(2)]
    for peer in peers:
        pl.semaphore_signal(barrier, inc=1, device_id=peer, device_id_type=MESH)
    return barrier, len(peers)


def send(src, dst, send_sem, recv_sem, peer):
    copy = pltpu.make_async_remote_copy(
        src_ref=src,
        dst_ref=dst,
        send_sem=send_sem,
        recv_sem=recv_sem,
        device_id=peer,
        device_id_type=MESH,
    )
    copy.start()


def await_bytes(ref, sem):
    pltpu.make_async_copy(ref, ref, sem).wait()


class Gather:
    def __init__(self, here, chunk, send_sem, near, far, group=lambda h: 0, part=None):
        self.here, self.chunk, self.send_sem = here, chunk, send_sem
        self.near, self.far, self.group, self.part = near, far, group, part

    def _send(self, origin, h, peer, recv_sem):
        ref = self.chunk(origin, h)
        send(ref, ref, self.send_sem, recv_sem, peer)

    def start(self, h):
        here = self.here
        mine = here.origin(0, False)
        self._send(mine, h, here.over_y(1), self.near.at[0, h])
        self._send(mine, h, here.over_y(-1), self.near.at[1, h])
        if self.part is None:
            self._send(mine, h, here.over_y(2), self.near.at[2, h])
        self._send(mine, h, here.other(), self.far.at[0, self.group(h)])

    def forward(self, h, between=None):
        here = self.here
        low, high = here.origin(-1, False), here.origin(1, False)
        await_bytes(self.chunk(low, h), self.near.at[0, h])
        self._pass(low, h, 0, here.over_y(1))
        self._send(low, h, here.other(), self.far.at[1, self.group(h)])
        if between is not None:
            between()
        await_bytes(self.chunk(high, h), self.near.at[1, h])
        self._pass(high, h, 1, here.over_y(-1))
        self._send(high, h, here.other(), self.far.at[2, self.group(h)])

    def _pass(self, origin, h, k, peer):
        if self.part is not None:
            ref = self.part(origin, h, k)
            send(ref, ref, self.send_sem, self.near.at[2 + k, h], peer)

    def last(self, h):
        here = self.here
        across = here.origin(2, False)
        if self.part is None:
            await_bytes(self.chunk(across, h), self.near.at[2, h])
        else:
            for k in range(2):
                await_bytes(self.part(across, h, k), self.near.at[2 + k, h])
        self._send(across, h, here.other(), self.far.at[3, self.group(h)])

    def finish(self, whole, g=0):
        here = self.here
        for k, dy in enumerate((0, -1, 1, 2)):
            await_bytes(whole(here.origin(dy, True)), self.far.at[k, g])


def slots_of(ids, here, total):
    tokens = ids.shape[0]
    lanes = lax.broadcasted_iota(jnp.int32, (tokens, 128), 1)
    named = [(lanes == ids[:, k : k + 1]).astype(F32) for k in range(2)]
    rows = lax.broadcasted_iota(jnp.int32, (tokens, tokens), 0)
    cols = lax.broadcasted_iota(jnp.int32, (tokens, tokens), 1)
    earlier = (cols < rows).astype(F32).astype(BF)
    before = jnp.dot(earlier, (named[0] + named[1]).astype(BF), preferred_element_type=F32)
    cap = total // (here.nz * NX)
    out = []
    for k in range(2):
        slot = jnp.sum(before * named[k], axis=1, keepdims=True)
        e = ids[:, k : k + 1]
        dz = ((e // NX if NX not in (1, 2, 4) else (e >> (NX.bit_length() - 1))) - here.z) & (here.nz - 1)
        dx = ((e & (NX - 1)) - here.x) & (NX - 1)
        out.append(((dz * NX + dx) * cap).astype(F32) + slot)
    return out


def nt(a, b):
    return lax.dot_general(a, b, (((1,), (1,)), ((), ())), preferred_element_type=F32)


def step_kernel(
    nz,
    og_hbm,
    x_hbm,
    rw_hbm,
    ids_hbm,
    conv_hbm,
    gb_hbm,
    gc_hbm,
    vv_hbm,
    taps_hbm,
    wg_hbm,
    wu_hbm,
    wd_hbm,
    op_hbm,
    go_ref,
    gradb_ref,
    gradc_ref,
    gradv_ref,
    gate_ref,
    up_ref,
    down_ref,
    og_ref,
    x_ref,
    rw_ref,
    ids_ref,
    conv_ref,
    gb_ref,
    gc_ref,
    vv_ref,
    taps_ref,
    sbuf,
    buf,
    wcat,
    wd,
    out_proj,
    gu,
    dhid_s,
    dcat,
    dt,
    part,
    pr,
    sb,
    ra,
    rb,
    sc,
    rc,
    fin,
    ret,
    pick,
    dh,
    dhall,
    dht,
    xall,
    mixed,
    mx,
    edge,
    halo,
    gpart,
    gr,
    i_sem,
    w_sem,
    own_sem,
    a_send,
    a_recv,
    g_send,
    g_near,
    g_far,
    pair_send,
    pair_recv,
    rs_send,
    rs_recv,
    sp_send,
    sp_recv,
    dh_send,
    dh_near,
    dh_far,
    xb_send,
    xb_near,
    xb_far,
    x_send,
    x_recv,
    m_send,
    m_recv,
    e_send,
    e_recv,
    z_send,
    z_recv,
):
    here = Place(nz)
    barrier, peers = greet(here)
    total, chans = sbuf.shape[1:]
    cap = total // (nz * NX)
    tokens = og_ref.shape[0]
    hid, padded = wg_hbm.shape[0], wd.shape[0]
    order = block_order(nz)
    at = {d: p for p, d in enumerate(order)}
    rows = NX * cap
    half = total // 2
    hb = nz // 2

    inputs = [
        pltpu.make_async_copy(a, b, i_sem.at[k])
        for k, (a, b) in enumerate(
            [
                (ids_hbm, ids_ref),
                (rw_hbm, rw_ref),
                (x_hbm, x_ref),
                (og_hbm, og_ref),
                (gb_hbm, gb_ref),
                (conv_hbm, conv_ref),
                (gc_hbm, gc_ref),
                (vv_hbm, vv_ref),
                (taps_hbm, taps_ref),
            ]
        )
    ]
    for load in inputs:
        load.start()
    loads = [
        pltpu.make_async_copy(wg_hbm, wcat.at[0:hid, :], w_sem.at[0]),
        pltpu.make_async_copy(wu_hbm, wcat.at[padded : padded + hid, :], w_sem.at[1]),
        pltpu.make_async_copy(wd_hbm, wd.at[0:hid, :], w_sem.at[2]),
        pltpu.make_async_copy(op_hbm, out_proj, w_sem.at[3]),
    ]
    for load in loads:
        load.start()

    inputs[0].wait()
    ids = ids_ref[...].astype(F32).T.astype(jnp.int32)
    slots = slots_of(ids, here, total)
    srow = lax.broadcasted_iota(jnp.int32, (total, tokens), 0).astype(F32)
    places = []
    for k in range(2):
        wide = jnp.broadcast_to(slots[k], (tokens, tokens)).T
        places.append((srow == wide[0:1, :]).astype(F32))
    both = (places[0] + places[1]).astype(BF)
    for load in inputs[1:4]:
        load.wait()
    rw = rw_ref[...].T
    sbuf[0] = jnp.dot(both, x_ref[...], preferred_element_type=F32).astype(BF)
    og = og_ref[...].astype(F32)
    dy = None
    for k in range(2):
        weighted = (rw[:, k : k + 1] * og).astype(BF)
        term = jnp.dot(places[k].astype(BF), weighted, preferred_element_type=F32)
        dy = term if dy is None else dy + term
    sbuf[1] = dy.astype(BF)

    def cols(origin):
        return pl.ds(pl.multiple_of(origin * chans, chans), chans)

    column = cols(here.tp)
    pl.semaphore_wait(barrier, peers)
    own = pltpu.make_async_copy(sbuf.at[:, 0:cap, :], buf.at[:, 0:cap, column], own_sem.at[5])
    own.start()
    for dz in [(-d) % nz for d in order]:
        for dx in range(NX):
            if dz or dx:
                r = (dz * NX + dx) * cap
                p = at[(-dz) % nz]
                t = p * rows + ((-dx) % NX) * cap
                send(
                    sbuf.at[:, pl.ds(r, cap), :],
                    buf.at[:, pl.ds(t, cap), column],
                    a_send,
                    a_recv.at[p],
                    here.over_sp(dz, dx),
                )
    scol = lax.broadcasted_iota(jnp.int32, (tokens, total), 1).astype(F32)
    pick[...] = ((scol == slots[0]).astype(F32) + (scol == slots[1]).astype(F32)).astype(BF)
    for load in inputs[4:]:
        load.wait()
    mixed[...] = (gb_ref[...].astype(F32) * conv_ref[...].astype(F32)).astype(BF)
    wcat[hid:padded, :] = jnp.zeros((padded - hid, wcat.shape[1]), BF)
    wcat[padded + hid :, :] = jnp.zeros((padded - hid, wcat.shape[1]), BF)
    wd[hid:, :] = jnp.zeros((padded - hid, wcat.shape[1]), BF)

    side = lax.rem(here.z, 2)
    family = [(dm, dx) for dm in range(2) for dx in range(NX) if dm or dx]
    seat = pl.ds(pl.multiple_of((side * NX + here.x) * tokens, tokens), tokens)
    own_mixed = pltpu.make_async_copy(mixed, mx.at[seat, :], own_sem.at[0])
    own_mixed.start()

    def chunk(origin, h):
        return buf.at[:, pl.ds(h * rows, rows), cols(origin)]

    def part_of(origin, h, k):
        return buf.at[k, pl.ds(h * rows, rows), cols(origin)]

    gather = Gather(here, chunk, g_send, g_near, g_far, lambda h: h // hb, part_of)

    def hidden_units(r0):
        r = pl.ds(r0, half)

        def ahead():
            gu[...] = nt(buf[0, r, :], wcat[...])

        def back():
            dhid_s[...] = nt(buf[1, r, :], wd[...])

        def combine():
            gate, upval, dhid = gu[:, :padded], gu[:, padded:], dhid_s[...]
            sig = jax.nn.sigmoid(gate)
            act = gate * sig
            dcat[r, 0:padded] = (dhid * upval * (sig * (1.0 + gate * (1.0 - sig)))).astype(BF)
            dcat[r, padded : 2 * padded] = (dhid * act).astype(BF)
            dcat[r, 2 * padded :] = (act * upval).astype(BF)

        return ahead, back, combine

    def whole(k):
        return lambda origin: buf.at[:, pl.ds(k * half, half), cols(origin)]

    def spread(k, first_y):
        r = pl.ds(k * half, half)
        d = dcat[r, 0 : 2 * padded]
        for y in range(first_y, first_y + 2):
            c = pl.ds(2 * y * chans, 2 * chans)
            part[r, c] = jnp.dot(d, wcat[:, c], preferred_element_type=F32).astype(BF)
        for y in range(first_y, first_y + 2):
            at = cols(2 * y + 1 - here.c)
            send(part.at[r, at], pr.at[y, r, :], pair_send, pair_recv.at[k], here.other())

    def pair(p, dy):
        y = lax.rem(here.y + dy + NY, NY)
        r = pl.ds(p * rows, rows)
        return part[r, cols(2 * y + here.c)].astype(F32) + pr[y, r, :].astype(F32)

    def stage_a(p):
        way = 1 if p % 2 == 0 else -1
        r = pl.ds(p * rows, rows)
        sb[0, r, :] = pair(p, 2).astype(BF)
        send(sb.at[0, r, :], ra.at[r, :], rs_send.at[0], rs_recv.at[0, p], here.over_y(way))
        sb[1, r, :] = pair(p, -way).astype(BF)
        send(sb.at[1, r, :], rb.at[r, :], rs_send.at[1], rs_recv.at[1, p], here.over_y(-way))

    def stage_b(p):
        way = 1 if p % 2 == 0 else -1
        r = pl.ds(p * rows, rows)
        await_bytes(ra.at[r, :], rs_recv.at[0, p])
        sc[r, :] = (pair(p, way) + ra[r, :].astype(F32)).astype(BF)
        send(sc.at[r, :], rc.at[r, :], rs_send.at[2], rs_recv.at[2, p], here.over_y(way))

    def stage_c(p):
        r = pl.ds(p * rows, rows)
        await_bytes(rb.at[r, :], rs_recv.at[1, p])
        await_bytes(rc.at[r, :], rs_recv.at[2, p])
        fin[r, :] = (pair(p, 0) + rb[r, :].astype(F32) + rc[r, :].astype(F32)).astype(BF)
        dz = order[p]
        for dx in range(NX):
            src = fin.at[pl.ds(p * rows + dx * cap, cap), :]
            t = (((-dz) % nz) * NX + (-dx) % NX) * cap
            dst = ret.at[pl.ds(t, cap), :]
            if dz or dx:
                send(src, dst, sp_send, sp_recv, here.over_sp(dz, dx))

    def pair_arrived(k):
        await_bytes(pr.at[:, pl.ds(k * half, half), :], pair_recv.at[k])

    first = list(range(hb - 1, -1, -1))
    second = list(range(hb, nz))
    for p in range(nz + LAST):
        if p < nz:
            if p == 0:
                own.wait()
                await_bytes(buf.at[:, cap:rows, column], a_recv.at[0])
            else:
                await_bytes(buf.at[:, pl.ds(p * rows, rows), column], a_recv.at[p])
            gather.start(p)
        if p == nz - 1:
            for dm, dx in family:
                send(mixed, mx.at[seat, :], m_send, m_recv, here.paired(dm, dx))
        if 0 <= p - FORWARD < nz:
            gather.forward(p - FORWARD, back if p == EXPERTS_AT + 1 else None)
        if p == EXPERTS_AT:
            gather.finish(whole(0), 0)
            for load in loads[:3]:
                load.wait()
            ahead, back, combine = hidden_units(0)
            ahead()
        if p == EXPERTS_AT + 1:
            combine()
        if 0 <= p - LAST < nz:
            gather.last(p - LAST)
        if p > EXPERTS_AT and p < EXPERTS_AT + 3:
            spread(0, 2 * (p - EXPERTS_AT - 1))
    pair_arrived(0)
    for p in first:
        stage_a(p)
    gather.finish(whole(1), 1)
    for task in hidden_units(half):
        task()
    spread(1, 0)
    spread(1, 2)
    for p in first:
        stage_b(p)
    pair_arrived(1)
    for p in second:
        stage_a(p)
    slab = 3 * padded // 9

    def turn(k):
        dt[k * slab : (k + 1) * slab, :] = dcat[:, k * slab : (k + 1) * slab].astype(F32).T.astype(BF)

    def weights(n):
        c = pl.ds(n * chans, chans)
        both = jnp.dot(dt[0 : 2 * padded, :], buf[0, :, c], preferred_element_type=F32)
        gate_ref[:, c] = both[0:hid, :].astype(BF)
        up_ref[:, c] = both[padded : padded + hid, :].astype(BF)
        down_ref[:, c] = jnp.dot(dt[2 * padded :, :], buf[1, :, c], preferred_element_type=F32)[0:hid, :].astype(BF)

    for p in first:
        stage_c(p)
    for k in range(9):
        turn(k)
    for p in second:
        stage_b(p)
    for p in second:
        stage_c(p)
    ret[0:cap, :] = fin[0:cap, :]
    for n in range(3):
        weights(n)
    await_bytes(ret.at[pl.ds(cap, total - cap), :], sp_recv)

    moe = jnp.dot(pick[...], ret[...], preferred_element_type=F32)
    grad_h = og_ref[...].astype(F32) + moe
    dht[...] = grad_h.T.astype(BF)
    dh[...] = grad_h.astype(BF)

    wide = chans // NX
    piece = wide // 2
    tcol = pl.ds(pl.multiple_of((side * NX + here.x) * tokens, tokens), tokens)

    def orows(origin, h=0, n=1):
        size = piece // n
        return pl.ds(pl.multiple_of(origin * piece + h * size, size), size)

    def share(m, x):
        return pl.ds(pl.multiple_of(x * wide + m * piece, piece), piece)

    mine = orows(here.tp)
    for dm, dx in family:
        m = lax.rem(side + dm, 2)
        send(
            dht.at[share(m, lax.rem(here.x + dx, NX)), :],
            xall.at[mine, tcol],
            x_send,
            x_recv,
            here.paired(dm, dx),
        )
    own_x = pltpu.make_async_copy(dht.at[share(side, here.x), :], xall.at[mine, tcol], own_sem.at[1])
    own_x.start()
    own_dh = pltpu.make_async_copy(dh, dhall.at[:, column], own_sem.at[2])
    own_dh.start()
    own_dh.wait()
    ht = tokens // 2
    dh_gather = Gather(here, lambda o, h: dhall.at[pl.ds(h * ht, ht), cols(o)], dh_send, dh_near, dh_far)
    xb_gather = Gather(here, lambda o, h: xall.at[orows(o, h, 2), :], xb_send, xb_near, xb_far)
    dh_gather.start(0)
    dh_gather.start(1)
    weights(3)
    own_x.wait()
    await_bytes(xall.at[pl.ds(0, piece), pl.ds(0, len(family) * tokens)], x_recv)
    xb_gather.start(0)
    xb_gather.start(1)
    weights(4)
    weights(5)
    for h in range(2):
        dh_gather.forward(h)
    for h in range(2):
        xb_gather.forward(h)
    for h in range(2):
        dh_gather.last(h)
    for h in range(2):
        xb_gather.last(h)
    dh_gather.finish(lambda o: dhall.at[:, cols(o)])
    loads[3].wait()
    grad_z = jnp.dot(dhall[...], out_proj[...], preferred_element_type=F32)
    dconv = (grad_z * gb_ref[...].astype(F32)).astype(BF)
    edge[0, :, :] = dconv[0:16, :]
    edge[1, :, :] = dconv[tokens - 16 :, :]
    last_sp = nz * NX
    before = (lax.rem(here.sp + last_sp - 1, last_sp), here.tp)
    after = (lax.rem(here.sp + 1, last_sp), here.tp)
    send(edge.at[0], halo.at[1], e_send.at[0], e_recv.at[1], before)
    send(edge.at[1], halo.at[0], e_send.at[1], e_recv.at[0], after)
    gradb_ref[...] = (grad_z * conv_ref[...].astype(F32)).astype(BF)
    own_mixed.wait()
    await_bytes(mx.at[pl.ds(0, len(family) * tokens), :], m_recv)
    xb_gather.finish(lambda o: xall.at[orows(o), :])
    gpart[...] = jnp.dot(xall[...], mx[...], preferred_element_type=F32).astype(BF)
    for dz in sorted(range(1, nz), key=lambda d: -min(d, nz - d)):
        to = lax.rem(here.z + dz, nz)
        send(gpart.at[orows(to), :], gr.at[dz], z_send, z_recv, here.over_sp(dz, 0))
    own_g = pltpu.make_async_copy(gpart.at[orows(here.z), :], gr.at[0], own_sem.at[4])
    own_g.start()

    for n in range(6, 2 * NY):
        weights(n)
    await_bytes(halo.at[0], e_recv.at[0])
    await_bytes(halo.at[1], e_recv.at[1])
    dconv = dconv.astype(F32)
    row = lax.broadcasted_iota(jnp.int32, dconv.shape, 0)
    low = halo[0].astype(F32)[15:16, :] * (here.sp > 0).astype(F32)
    high = halo[1].astype(F32)[0:1, :] * (here.sp < last_sp - 1).astype(F32)
    prev = jnp.where(row == 0, low, pltpu.roll(dconv, 1, 0))
    nxt = jnp.where(row == tokens - 1, high, pltpu.roll(dconv, tokens - 1, 0))
    grad_u = taps_ref[0:1, :] * nxt + taps_ref[1:2, :] * dconv + taps_ref[2:3, :] * prev
    gradc_ref[...] = (grad_u * vv_ref[...].astype(F32)).astype(BF)
    gradv_ref[...] = (grad_u * gc_ref[...].astype(F32)).astype(BF)

    others = 2 * NY - 1
    await_bytes(sbuf.at[:, pl.ds(0, total - cap), :], a_send)
    await_bytes(buf.at[:, pl.ds(0, total - total // (2 * NY)), :], g_send)
    await_bytes(pr, pair_send)
    for k in range(3):
        await_bytes(ra, rs_send.at[k])
    await_bytes(ret.at[pl.ds(cap, total - cap), :], sp_send)
    await_bytes(dhall.at[:, pl.ds(0, others * chans)], dh_send)
    await_bytes(xall.at[pl.ds(0, others * piece), :], xb_send)
    await_bytes(xall.at[pl.ds(0, piece), pl.ds(0, len(family) * tokens)], x_send)
    await_bytes(mx.at[pl.ds(0, len(family) * tokens), :], m_send)
    await_bytes(edge.at[0], e_send.at[0])
    await_bytes(edge.at[1], e_send.at[1])

    own_g.wait()
    await_bytes(gr.at[pl.ds(1, nz - 1)], z_recv)
    for m in range(2):
        summed = gr[m].astype(F32)
        for k in range(m + 2, nz, 2):
            summed = summed + gr[k].astype(F32)
        go_ref[pl.ds(pl.multiple_of(lax.rem(side + m, 2) * piece, piece), piece), :] = summed
    await_bytes(gr.at[pl.ds(1, nz - 1)], z_send)


def write_kernel(*refs):
    count = len(refs) // 2
    sems = refs[-1]
    copies = [pltpu.make_async_copy(refs[k], refs[count + k], sems.at[k]) for k in range(count)]
    for copy in copies:
        copy.start()
    for copy in copies:
        copy.wait()


VM = pl.BlockSpec(memory_space=pltpu.VMEM)
ANY = pl.BlockSpec(memory_space=pl.ANY)
FORWARD, LAST = 2, 4
EXPERTS_AT = 8


def local(
    nz,
    ntp,
    out_grad,
    moe_input,
    route_weight,
    route_ids,
    gate_proj,
    up_proj,
    down_proj,
    out_proj,
    conv_out,
    gate_b,
    gate_c,
    value_v,
    conv_taps,
):
    tokens, chans = out_grad.shape
    ns = nz * NX
    cap = 4 * tokens // ns
    total = ns * cap
    width = chans * ntp
    hid = gate_proj.shape[2]
    padded = -(-hid // 128) * 128
    wide = chans // NX
    dma = pltpu.SemaphoreType.DMA

    def vm(*shape):
        return pltpu.VMEM(shape, BF)

    small = [
        jax.ShapeDtypeStruct((wide, chans), F32),
        jax.ShapeDtypeStruct((tokens, chans), BF),
        jax.ShapeDtypeStruct((tokens, chans), BF),
        jax.ShapeDtypeStruct((tokens, chans), BF),
    ]
    held = [(a.shape, a.dtype) for a in small]
    held += [((hid, width), BF)] * 3
    results = pl.pallas_call(
        functools.partial(step_kernel, nz),
        out_shape=[pltpu.VMEM(*h) for h in held],
        in_specs=[ANY] * 13,
        out_specs=[VM] * 7,
        scratch_shapes=[
            vm(tokens, chans),
            vm(tokens, chans),
            pltpu.VMEM((2, tokens), F32),
            pltpu.VMEM((2, tokens), jnp.int32),
            vm(tokens, chans),
            vm(tokens, chans),
            vm(tokens, chans),
            vm(tokens, chans),
            pltpu.VMEM(conv_taps.shape, F32),
            vm(2, total, chans),
            vm(2, total, width),
            vm(2 * padded, width),
            vm(padded, width),
            vm(width, chans),
            pltpu.VMEM((total // 2, 2 * padded), F32),
            pltpu.VMEM((total // 2, padded), F32),
            vm(total, 3 * padded),
            vm(3 * padded, total),
            vm(total, width),
            vm(NY, total, chans),
            vm(2, total, chans),
            vm(total, chans),
            vm(total, chans),
            vm(total, chans),
            vm(total, chans),
            vm(total, chans),
            vm(total, chans),
            vm(tokens, total),
            vm(tokens, chans),
            vm(tokens, width),
            vm(chans, tokens),
            vm(ntp * wide // 2, 2 * NX * tokens),
            vm(tokens, chans),
            vm(2 * NX * tokens, chans),
            vm(2, 16, chans),
            vm(2, 16, chans),
            vm(nz * wide // 2, chans),
            vm(nz, wide // 2, chans),
            dma((9,)),
            dma((4,)),
            dma((7,)),
            dma,
            dma((nz,)),
            dma,
            dma((4, nz)),
            dma((4, 2)),
            dma,
            dma((2,)),
            dma((3,)),
            dma((3, nz)),
            dma,
            dma,
            dma,
            dma((3, 2)),
            dma((4, 1)),
            dma,
            dma((3, 2)),
            dma((4, 1)),
            dma,
            dma,
            dma,
            dma,
            dma((2,)),
            dma((2,)),
            dma,
            dma,
        ],
        compiler_params=pltpu.CompilerParams(
            collective_id=0, has_side_effects=True, vmem_limit_bytes=40 * 1024 * 1024
        ),
        name="step",
    )(
        *(
            pltpu.with_memory_space_constraint(a, pltpu.HBM)
            for a in (
                out_grad,
                moe_input,
                route_weight.T,
                route_ids.T,
                conv_out,
                gate_b,
                gate_c,
                value_v,
                conv_taps,
                gate_proj[0].T,
                up_proj[0].T,
                down_proj[0],
                out_proj,
            )
        )
    )
    grad_out, grad_b, grad_c, grad_v, grad_gate, grad_up, grad_down = pl.pallas_call(
        write_kernel,
        out_shape=[jax.ShapeDtypeStruct(*h) for h in held],
        in_specs=[VM] * 7,
        out_specs=[ANY] * 7,
        scratch_shapes=[dma((7,))],
        compiler_params=pltpu.CompilerParams(vmem_limit_bytes=8 * 1024 * 1024),
        name="write",
    )(*[pltpu.with_memory_space_constraint(r, pltpu.VMEM) for r in results])
    return (grad_gate.T[None], grad_up.T[None], grad_down[None], grad_out, grad_b, grad_c, grad_v)


def solution(mesh):
    nz = mesh.shape["sp"] // NX
    ntp = mesh.shape["tp"]
    tok, tok_tp = P("sp", None), P("sp", "tp")
    return jax.shard_map(
        functools.partial(local, nz, ntp),
        mesh=mesh,
        in_specs=(
            tok_tp,
            tok_tp,
            tok,
            tok,
            P("sp", None, "tp"),
            P("sp", None, "tp"),
            P("sp", "tp", None),
            P(None, "tp"),
            tok_tp,
            tok_tp,
            tok_tp,
            tok_tp,
            P(None, "tp"),
        ),
        out_specs=(
            P("sp", None, "tp"),
            P("sp", None, "tp"),
            P("sp", "tp", None),
            tok_tp,
            tok_tp,
            tok_tp,
            tok_tp,
        ),
        check_vma=False,
    )
```
